512 devices in a mesh: ep: 32 (over z, core), tp: 16 (over y, x).
Axes of the slice: x: 4, y: 4, z: 16, core: 2. Of those that a mesh axis runs over, the one named last changes fastest.
Arguments:
- mix_in: bfloat16 [4096, 2048], P('ep'), may hold values from -6 to 6
- mix_gain: float32 [2048], replicated, may hold values from 0.1 to 1.9
- lam_re: float32 [128, 64], P('tp'), may hold values from -0.34 to -1e-05
- lam_im: float32 [128, 64], P('tp'), may hold values from 0.2 to 4
- log_dt: float32 [128], P('tp'), may hold values from -2.31 to 0
- b_re: float32 [128, 64, 16], P('tp'), may hold values from -0.0625 to 0.0625
- b_im: float32 [128, 64, 16], P('tp'), may hold values from -0.0625 to 0.0625
- c_re: float32 [128, 16, 64], P('tp'), may hold values from -0.5 to 0.5
- c_im: float32 [128, 16, 64], P('tp'), may hold values from -0.5 to 0.5
- d_skip: float32 [2048], P('tp'), may hold values from -2 to 2
- log_retain: float32 [4096, 128], P('ep', 'tp'), may hold values from -2.2 to 0
- w_lin: bfloat16 [2048, 2048], P(None, 'tp'), may hold values from -0.125 to 0.125
- w_glu: bfloat16 [2048, 2048], P(None, 'tp'), may hold values from -0.125 to 0.125
- moe_in: bfloat16 [4096, 2048], P('ep'), may hold values from -6 to 6
- moe_gain: float32 [2048], replicated, may hold values from 0.1 to 1.9
- routes: int32 [4096, 2], P('ep'), may hold values from 0 to 31, all different within a row; in each aligned block of 128 rows (0 to 127, 128 to 255, ...) at most 12 rows name the same one
- route_weight: float32 [4096, 2], P('ep'), may hold values from 0.1 to 1
- w_gate: bfloat16 [32, 2048, 4096], P('ep', None, 'tp'), may hold values from -0.125 to 0.125
- w_up: bfloat16 [32, 2048, 4096], P('ep', None, 'tp'), may hold values from -0.125 to 0.125
- w_down: bfloat16 [32, 4096, 2048], P('ep', 'tp'), may hold values from -0.09375 to 0.09375
Outputs:
- mix_out: bfloat16 [4096, 2048], P('ep', 'tp')
- moe_out: bfloat16 [4096, 2048], P('ep', 'tp')
The draws below stay inside these ranges and needn't reach their ends.
Inputs may be any that keep to these rules, and one draw needn't show every extreme that they name: `routes`: each row names 2 different experts. In each aligned block of 128 rows (the rows of one index of ep) no expert is named by more than 12 rows, and in some block an expert is named by exactly 12 rows.
All inputs are finite; a program needn't handle non-finite values.
Results may differ from the reference program's by a relative error of at most 0.015.
Values may be sent and summed in bfloat16 or wider, within the bound.
A program may use at most 128 MiB of HBM per device.

```python
import math
import jax
import jax.numpy as jnp
import numpy as np
from jax import lax

D = 2048
GROUP_CH = 16
STATE = 64
H = 4096
TOP = 2
TA_DEV = 128
TB_DEV = 128
GROUPS = 128
EXPERTS = 32
CAP = 12
TOKA = 4096
TOKB = 4096
N_EP = 32
N_TP = 16


def shared_steps(key):
    step_key = jax.random.fold_in(key, 11)
    return jax.random.uniform(step_key, (GROUPS,), jnp.float32, math.log(0.1), 0.0)


def draw_log_dt(key, part):
    return shared_steps(key)


def draw_lam_re(key, part):
    time_step = jnp.exp(shared_steps(key))[:, None]
    slow_share = 0.5
    chooser = jax.random.uniform(jax.random.fold_in(key, 12), (GROUPS, STATE), jnp.float32)
    slow_rate = jnp.exp(jax.random.uniform(jax.random.fold_in(key, 13), (GROUPS, STATE), jnp.float32, math.log(1e-05), math.log(5e-05)))
    fast_rate = jnp.exp(jax.random.uniform(jax.random.fold_in(key, 14), (GROUPS, STATE), jnp.float32, math.log(0.01), math.log(0.033)))
    rate = jnp.where(chooser < slow_share, slow_rate, fast_rate)
    return -rate / time_step


def draw_log_retain(key, part):
    blocks = TOKA // TA_DEV
    steady_rate = jnp.exp(jax.random.uniform(jax.random.fold_in(key, 21), (blocks, 1, GROUPS), jnp.float32, math.log(0.3), math.log(1.2))) / TOKA
    stable_level = -jnp.broadcast_to(steady_rate, (blocks, TA_DEV, GROUPS)).reshape(TOKA, GROUPS)
    spots = jax.random.randint(jax.random.fold_in(key, 22), (3, GROUPS), 0, TOKA)
    loss_values = jnp.log(jax.random.uniform(jax.random.fold_in(key, 23), (3, GROUPS), jnp.float32, 0.5, 0.8))
    spot_matches = jnp.arange(TOKA, dtype=jnp.int32)[:, None, None] == spots[None]
    token_spurts = jnp.sum(jnp.where(spot_matches, loss_values[None], 0.0), axis=1)
    return stable_level + token_spurts


def block_scale(stream_key, extent, cuts, least, largest):
    loudness = 1.0
    for axis_at, blocks in cuts:
        heights = jax.random.uniform(jax.random.fold_in(jax.random.fold_in(stream_key, 6), axis_at), (blocks,), jnp.float32, least / len(cuts), largest / len(cuts))
        loudness = loudness * jnp.repeat(jnp.exp(heights), extent[axis_at] // blocks).reshape((-1,) + (1,) * (len(extent) - 1 - axis_at))
    return loudness


def assign_block(rng, own, number, rows, number_of, top, reach, lean):
    ranking = jax.random.permutation(rng, number_of)
    heavy_load, usual = shares(number_of, rows * top, reach, lean, True), shares(number_of, rows * top, reach, lean, False)
    places = jnp.arange(number_of)

    def named(tallies, offset_by):
        used = int((tallies > 0).sum())
        fixed = max(1, used // 4)
        moved = fixed + (places - fixed + offset_by * (used - fixed)) % max(1, number_of - fixed)
        return jnp.zeros((number_of,), jnp.int32).at[ranking[jnp.where(places < fixed, places, moved)]].set(jnp.asarray(tallies, jnp.int32))

    tallies = jnp.where(number % 4 == 0, named(heavy_load, number // 4), named(usual, number - number // 4 - 1))
    mixed = jax.random.permutation(jax.random.fold_in(own, 3), number_of)
    source_of, receiver = mixed[0:number_of // 2 * 2:2], mixed[1:number_of // 2 * 2:2]
    slack = jnp.minimum(tallies[source_of] - 1, reach - tallies[receiver]) // 2
    slack = jnp.where((source_of == ranking[0]) | (receiver == ranking[0]) | (tallies[receiver] == 0), 0, jnp.maximum(slack, 0))
    moved = jax.random.randint(jax.random.fold_in(own, 4), (number_of // 2,), 0, 1 << 20) % (slack + 1)
    tallies = tallies.at[source_of].add(-moved).at[receiver].add(moved)
    members = jnp.searchsorted(jnp.cumsum(tallies), jnp.arange(rows * top), side="right").astype(jnp.int32)
    listing = members.reshape(top, rows).T
    listing = listing[jax.random.permutation(jax.random.fold_in(own, 1), rows)]
    offset_by = jax.random.randint(jax.random.fold_in(own, 2), (rows, 1), 0, top)
    return jnp.take_along_axis(listing, (jnp.arange(top)[None, :] + offset_by) % top, axis=1)


def shares(count, total, bound, lean, full):
    weights = [(1 << 20) // math.isqrt(grade ** lean) + 1 for grade in range(1, count + 1)]
    largest = bound if full else min(bound, max(-(-total // count), total * weights[0] // sum(weights)))
    least = 1 if total - largest >= count - 1 else 0
    given, rest = [largest] + [least] * (count - 1), total - largest - least * (count - 1)
    while rest > 0:
        candidates = [i for i in range(1, count) if given[i] < largest] or [i for i in range(1, count) if given[i] < bound]
        pool, remaining = sum([weights[i] for i in candidates]), rest
        for i in candidates:
            extra = min(bound - given[i], max(1, remaining * weights[i] // pool), rest)
            given[i] = given[i] + extra
            rest = rest - extra
    return np.array(given)


def centred(rng, extent, width, limit, split=(), held_as=jnp.bfloat16):
    entries = jax.random.normal(rng, extent, jnp.float32) * width
    if len(split) > 0:
        entries = block_scale(rng, extent, split, -0.22, 0.18) * entries
    return jnp.clip(entries, min=-limit, max=limit).astype(held_as)


def setup_inputs(seed: int = 0) -> dict:
    streams_of = jax.random.split(jax.random.key(seed), 21)
    mix_in = centred(streams_of[0], (TOKA, D), 1.0, 6.0, ((0, 32),))
    mix_gain = jnp.clip(1.0 + 0.18 * jax.random.normal(streams_of[1], (D,), jnp.float32), 0.1, 1.9)
    lam_re = draw_lam_re(jax.random.fold_in(streams_of[20], 71), 0)
    lam_im = jnp.clip(0.2 + 3.8 * jax.random.uniform(streams_of[3], (GROUPS, STATE), jnp.float32) ** block_scale(streams_of[3], (GROUPS, STATE), ((0, 16),), -0.2, 0.2), 0.2, 4.0)
    log_dt = draw_log_dt(jax.random.fold_in(streams_of[20], 71), 0)
    b_re = centred(streams_of[5], (GROUPS, STATE, GROUP_CH), (GROUP_CH * TOKA // 8) ** -0.5, 0.0625, ((0, 16),), jnp.float32)
    b_im = centred(streams_of[6], (GROUPS, STATE, GROUP_CH), (GROUP_CH * TOKA // 8) ** -0.5, 0.0625, ((0, 16),), jnp.float32)
    c_re = centred(streams_of[7], (GROUPS, GROUP_CH, STATE), (2 * STATE) ** -0.5, 0.5, ((0, 16),), jnp.float32)
    c_im = centred(streams_of[8], (GROUPS, GROUP_CH, STATE), (2 * STATE) ** -0.5, 0.5, ((0, 16),), jnp.float32)
    d_skip = centred(streams_of[9], (D,), 0.5, 2.0, ((0, 16),), jnp.float32)
    log_retain = draw_log_retain(jax.random.fold_in(streams_of[20], 71), 0)
    w_lin = centred(streams_of[11], (D, D), D ** -0.5, 0.125, ((1, 16),))
    w_glu = centred(streams_of[12], (D, D), D ** -0.5, 0.125, ((1, 16),))
    moe_in = centred(streams_of[13], (TOKB, D), 1.0, 6.0, ((0, 32),))
    moe_gain = jnp.clip(1.0 + 0.18 * jax.random.normal(streams_of[14], (D,), jnp.float32), 0.1, 1.9)
    routes_keys = jax.random.split(jax.random.fold_in(streams_of[15], 1), TOKB // TB_DEV)
    routes_turns = jax.random.permutation(jax.random.fold_in(streams_of[15], 3), TOKB // TB_DEV)
    routes = jax.vmap(lambda own, number: assign_block(jax.random.fold_in(streams_of[15], 2), own, number, TB_DEV, EXPERTS, TOP, CAP, 2))(routes_keys, routes_turns).reshape((TOKB, TOP))
    route_weight = jnp.clip(jnp.exp(math.log(1.0) - 2.3025851 * jax.random.uniform(streams_of[16], (TOKB, TOP), jnp.float32) ** block_scale(streams_of[16], (TOKB, TOP), ((0, 32),), -0.2, 0.2)), 0.1, 1.0)
    w_gate = centred(streams_of[17], (EXPERTS, D, H), D ** -0.5, 0.125, ((0, 32), (2, 16)))
    w_up = centred(streams_of[18], (EXPERTS, D, H), D ** -0.5, 0.125, ((0, 32), (2, 16)))
    w_down = centred(streams_of[19], (EXPERTS, H, D), H ** -0.5, 0.09375, ((0, 32), (1, 16)))
    return {"mix_in": mix_in, "mix_gain": mix_gain, "lam_re": lam_re, "lam_im": lam_im, "log_dt": log_dt, "b_re": b_re, "b_im": b_im, "c_re": c_re, "c_im": c_im, "d_skip": d_skip, "log_retain": log_retain, "w_lin": w_lin, "w_glu": w_glu, "moe_in": moe_in, "moe_gain": moe_gain, "routes": routes, "route_weight": route_weight, "w_gate": w_gate, "w_up": w_up, "w_down": w_down}


EPS = 1e-06
HIGHEST = lax.Precision.HIGHEST

def root_mean_normed(values, gain):
    broadened_rows = values.astype(jnp.float32)
    inverse = lax.rsqrt(lax.optimization_barrier(jnp.mean(broadened_rows * broadened_rows, axis=-1, keepdims=True)) + EPS)
    return (broadened_rows * inverse * gain.astype(jnp.float32)).astype(jnp.bfloat16)

def compose(earlier, later):
    early_re, early_im, shift_re, shift_im = earlier
    late_re, late_im, offset_re, offset_im = later
    return (late_re * early_re - late_im * early_im, late_re * early_im + late_im * early_re, late_re * shift_re - late_im * shift_im + offset_re, late_re * shift_im + late_im * shift_re + offset_im)

def discretize(lam_re, lam_im, log_dt, b_re, b_im):
    time_step = jnp.exp(log_dt)[:, None]
    log_mag = lam_re * time_step
    angle = lam_im * time_step
    half_sine = jnp.sin(0.5 * angle)
    minus_re = jnp.expm1(log_mag) * jnp.cos(angle) - 2.0 * half_sine * half_sine
    minus_im = jnp.exp(log_mag) * jnp.sin(angle)
    denom = lam_re * lam_re + lam_im * lam_im
    coef_re = (minus_re * lam_re + minus_im * lam_im) / denom
    coef_im = (minus_im * lam_re - minus_re * lam_im) / denom
    drive_re = coef_re[..., None] * b_re - coef_im[..., None] * b_im
    drive_im = coef_re[..., None] * b_im + coef_im[..., None] * b_re
    return (log_mag, angle, drive_re, drive_im)

def local_scan(inputs, retain, log_mag, angle, drive_re, drive_im):
    length = inputs.shape[0]
    groups, states, channels = drive_re.shape
    broadened_rows = inputs.astype(jnp.float32).reshape(length, groups, channels)
    push_re = jnp.einsum('tgn,gpn->tgp', broadened_rows, drive_re, precision=HIGHEST).reshape(length, groups * states)
    push_im = jnp.einsum('tgn,gpn->tgp', broadened_rows, drive_im, precision=HIGHEST).reshape(length, groups * states)
    magnitude = jnp.exp(log_mag[None] + retain[:, :, None]).reshape(length, groups * states)
    decay_re = magnitude * jnp.cos(angle).reshape(1, groups * states)
    decay_im = magnitude * jnp.sin(angle).reshape(1, groups * states)
    return lax.associative_scan(compose, (decay_re, decay_im, push_re, push_im), axis=0)

def read_out(total_re, total_im, inputs, c_re, c_im, d_skip):
    length = inputs.shape[0]
    groups, channels, states = c_re.shape
    state_re = total_re.reshape(length, groups, states)
    state_im = total_im.reshape(length, groups, states)
    mixed = jnp.einsum('tgp,gnp->tgn', state_re, c_re, precision=HIGHEST)
    mixed = mixed - jnp.einsum('tgp,gnp->tgn', state_im, c_im, precision=HIGHEST)
    skipped = mixed.reshape(length, groups * channels) + d_skip * inputs.astype(jnp.float32)
    return jax.nn.gelu(skipped).astype(jnp.bfloat16)

def reference(mix_in, mix_gain, lam_re, lam_im, log_dt, b_re, b_im, c_re, c_im, d_skip, log_retain, w_lin, w_glu, moe_in, moe_gain, routes, route_weight, w_gate, w_up, w_down):
    normed = root_mean_normed(mix_in, mix_gain)
    log_mag, angle, drive_re, drive_im = discretize(lam_re, lam_im, log_dt, b_re, b_im)
    block_inputs = normed.reshape(TOKA // TA_DEV, TA_DEV, D)
    block_retain = log_retain.reshape(TOKA // TA_DEV, TA_DEV, GROUPS)

    def advance(carry, pieces):
        carry_re, carry_im = carry
        inputs, retain = pieces
        pref_re, pref_im, local_re, local_im = local_scan(inputs, retain, log_mag, angle, drive_re, drive_im)
        total_re = local_re + pref_re * carry_re - pref_im * carry_im
        total_im = local_im + pref_re * carry_im + pref_im * carry_re
        return ((total_re[-1], total_im[-1]), read_out(total_re, total_im, inputs, c_re, c_im, d_skip))
    anchor = jnp.zeros((GROUPS * STATE,), jnp.float32)
    _, blocks_out = lax.scan(advance, (anchor, anchor), (block_inputs, block_retain))
    activated = blocks_out.reshape(TOKA, D)
    mix_lin = jnp.dot(activated, w_lin, preferred_element_type=jnp.float32)
    mix_glu = jnp.dot(activated, w_glu, preferred_element_type=jnp.float32)
    mix_out = (mix_lin * jax.nn.sigmoid(mix_glu)).astype(jnp.bfloat16)
    normed_b = root_mean_normed(moe_in, moe_gain)
    flat_routes = routes.reshape(-1)
    assigns = flat_routes.shape[0]
    padded = jnp.concatenate([normed_b, jnp.zeros((1, D), jnp.bfloat16)], axis=0)

    def expert_rows(table, expert):
        picks = jnp.nonzero(flat_routes == expert, size=CAP * N_EP, fill_value=assigns)[0].astype(jnp.int32)
        chosen = padded[picks // TOP]
        gate_pre = jnp.dot(chosen, w_gate[expert], preferred_element_type=jnp.float32)
        up_pre = jnp.dot(chosen, w_up[expert], preferred_element_type=jnp.float32)
        hidden = (jax.nn.silu(gate_pre) * up_pre).astype(jnp.bfloat16)
        blocked = hidden.reshape(-1, N_TP, H // N_TP).astype(jnp.float32)
        down_blocks = w_down[expert].reshape(N_TP, H // N_TP, D).astype(jnp.float32)
        partials = jnp.einsum('rkh,khd->rkd', blocked, down_blocks).astype(jnp.bfloat16)
        partials = lax.optimization_barrier(partials)
        result = lax.optimization_barrier(jnp.sum(partials.astype(jnp.float32), axis=1)).astype(jnp.bfloat16)
        return (table.at[picks].set(result), None)
    opening_lookup = jnp.zeros((assigns + 1, D), jnp.bfloat16)
    table, _ = lax.scan(expert_rows, opening_lookup, jnp.arange(EXPERTS, dtype=jnp.int32))
    gathered = table[:assigns].reshape(TOKB, TOP, D).astype(jnp.float32)
    moe_out = lax.optimization_barrier(jnp.sum(gathered * route_weight[:, :, None], axis=1)).astype(jnp.bfloat16)
    return (mix_out, moe_out)
```

```python
import jax
import jax.numpy as jnp
from jax import lax
from jax.sharding import Mesh
from jax.sharding import PartitionSpec as P

EP = ("ep_0", "ep_1")


EPS = 1e-06
HIGHEST = lax.Precision.HIGHEST


def filled_with(array, identity):
    return jax.tree.map(
        lambda part, zero: jnp.zeros_like(part) + jnp.asarray(zero, part.dtype), array, identity
    )


def all_in_one(array, axis):
    leaves = jax.tree.leaves(array)
    order = sorted(range(len(leaves)), key=lambda k: -leaves[k].size)
    width = (1, *leaves[order[0]].shape)[-1]
    lines = [
        jnp.pad(leaves[k].reshape(-1), (0, -leaves[k].size % width)).reshape(-1, width)
        for k in order
    ]
    both, at, found = (lax.all_gather(jnp.concatenate(lines), axis), 0, {})
    for k, line in zip(order, lines):
        slab = both[:, at : at + len(line)].reshape(len(both), -1)
        found[k] = slab[:, : leaves[k].size].reshape(-1, *leaves[k].shape)
        at += len(line)
    numbers = iter(range(len(leaves)))
    return jax.tree.map(lambda _: found[next(numbers)], array)


def entering(array, axes, combine, identity):
    before = start = filled_with(array, identity)
    subtotal = array
    for axis in reversed(axes):
        length, here = (lax.axis_size(axis), lax.axis_index(axis))
        pieces = all_in_one(subtotal, axis)
        inside, subtotal = (start, start)
        for k in range(length):
            passed = k < here
            subtotal = combine(subtotal, jax.tree.map(lambda part: part[k], pieces))
            inside = jax.tree.map(lambda new, old: jnp.where(passed, new, old), subtotal, inside)
        before = combine(inside, before)
    return before


def laid_out(pieces, dim):
    lengths = list(pieces.shape[1:])
    lengths[dim] *= pieces.shape[0]
    return jnp.moveaxis(pieces, 0, dim).reshape(lengths)


def from_everyone(array, axis):
    copies = jnp.broadcast_to(array, (lax.axis_size(axis), *array.shape))
    return lax.all_to_all(copies, axis, split_axis=0, concat_axis=0, tiled=True)


def gather_directly(array, axis, dim):
    return laid_out(from_everyone(array, axis), dim)


def in_blocks(array, dim, length):
    before, after = (array.shape[:dim], array.shape[dim + 1 :])
    return jnp.moveaxis(array.reshape(*before, length, -1, *after), dim, 0)


def sent_and_summed(array, axis, dim):
    pieces = in_blocks(array, dim, lax.axis_size(axis))
    arrived = lax.all_to_all(pieces, axis, split_axis=0, concat_axis=0, tiled=True)
    return arrived.astype(jnp.float32).sum(axis=0)


def root_mean_normed(values, gain):
    broadened_rows = values.astype(jnp.float32)
    inverse = lax.rsqrt(jnp.mean(broadened_rows * broadened_rows, axis=-1, keepdims=True) + EPS)
    return (broadened_rows * inverse * gain).astype(jnp.bfloat16)


def compose(earlier, later):
    early_re, early_im, shift_re, shift_im = earlier
    late_re, late_im, offset_re, offset_im = later
    return (
        late_re * early_re - late_im * early_im,
        late_re * early_im + late_im * early_re,
        late_re * shift_re - late_im * shift_im + offset_re,
        late_re * shift_im + late_im * shift_re + offset_im,
    )


def discretize(lam_re, lam_im, log_dt, b_re, b_im):
    time_step = jnp.exp(log_dt)[:, None]
    log_mag = lam_re * time_step
    angle = lam_im * time_step
    half_sine = jnp.sin(0.5 * angle)
    minus_re = jnp.expm1(log_mag) * jnp.cos(angle) - 2.0 * half_sine * half_sine
    minus_im = jnp.exp(log_mag) * jnp.sin(angle)
    denom = lam_re * lam_re + lam_im * lam_im
    coef_re = (minus_re * lam_re + minus_im * lam_im) / denom
    coef_im = (minus_im * lam_re - minus_re * lam_im) / denom
    drive_re = coef_re[..., None] * b_re - coef_im[..., None] * b_im
    drive_im = coef_re[..., None] * b_im + coef_im[..., None] * b_re
    return (log_mag, angle, drive_re, drive_im)


def block_scan(inputs, retain, log_mag, angle, drive_re, drive_im):
    length = inputs.shape[0]
    groups, states, channels = drive_re.shape
    broadened_rows = inputs.astype(jnp.float32).reshape(length, groups, channels)
    push_re = jnp.einsum("tgn,gpn->gtp", broadened_rows, drive_re, precision=HIGHEST)
    push_im = jnp.einsum("tgn,gpn->gtp", broadened_rows, drive_im, precision=HIGHEST)
    steps = jnp.arange(length, dtype=jnp.float32)
    causal = steps[:, None] >= steps[None, :]
    summed = jnp.dot(causal.astype(jnp.float32), retain, precision=HIGHEST)
    rows = summed.T
    gaps = jnp.minimum(rows[:, :, None] - rows[:, None, :], 0.0)
    kept = jnp.where(causal[None], jnp.exp(gaps), 0.0)
    centred = (steps - length // 2)[None, :, None]
    growth = log_mag[:, None, :] * centred
    turn = angle[:, None, :] * centred
    cosine = jnp.cos(turn)
    sine = jnp.sin(turn)
    up_re = jnp.exp(growth) * cosine
    up_im = jnp.exp(growth) * sine
    down_re = jnp.exp(-growth) * cosine
    down_im = -jnp.exp(-growth) * sine
    seed_re = push_re * down_re - push_im * down_im
    seed_im = push_re * down_im + push_im * down_re
    seeds = jnp.concatenate([seed_re, seed_im], axis=2)
    held = jnp.einsum("gts,gsp->gtp", kept, seeds, precision=HIGHEST)
    fade = jnp.exp(rows)[:, :, None]
    return (held[..., :states], held[..., states:], up_re, up_im, fade)


def power_of(log_mag, angle, exponent):
    magnitude = jnp.exp(log_mag * exponent)
    return (magnitude * jnp.cos(angle * exponent), magnitude * jnp.sin(angle * exponent))


def read_out(state_re, state_im, inputs, c_re, c_im, d_skip):
    length = inputs.shape[0]
    groups, channels, states = c_re.shape
    states_both = jnp.concatenate([state_re, state_im], axis=2)
    c_both = jnp.concatenate([c_re, -c_im], axis=2)
    mixed = jnp.einsum("gtp,gnp->tgn", states_both, c_both, precision=HIGHEST)
    skipped = mixed.reshape(length, groups * channels) + d_skip * inputs.astype(jnp.float32)
    return jax.nn.gelu(skipped).astype(jnp.bfloat16)


def local(
    mix_in,
    mix_gain,
    lam_re,
    lam_im,
    log_dt,
    b_re,
    b_im,
    c_re,
    c_im,
    d_skip,
    log_retain,
    w_lin,
    w_glu,
    moe_in,
    moe_gain,
    routes,
    route_weight,
    w_gate,
    w_up,
    w_down,
):
    normed = root_mean_normed(mix_in, mix_gain)
    channels_here = d_skip.shape[0]
    own_inputs = lax.dynamic_slice_in_dim(
        normed, lax.axis_index("tp") * channels_here, channels_here, 1
    )
    log_mag, angle, drive_re, drive_im = discretize(lam_re, lam_im, log_dt, b_re, b_im)
    held_re, held_im, up_re, up_im, fade = block_scan(
        own_inputs, log_retain, log_mag, angle, drive_re, drive_im
    )
    length = own_inputs.shape[0]
    end_re = (up_re * held_re - up_im * held_im)[:, -1]
    end_im = (up_re * held_im + up_im * held_re)[:, -1]
    whole_re, whole_im = power_of(log_mag, angle, float(length))
    pref_re = fade[:, -1] * whole_re
    pref_im = fade[:, -1] * whole_im
    flat = [part.reshape(-1) for part in (pref_re, pref_im, end_re, end_im)]
    unity = jnp.ones_like(flat[0])
    nought = jnp.zeros_like(flat[0])
    incoming = entering(tuple(flat), EP, compose, (unity, nought, nought, nought))
    carry_re = incoming[2].reshape(pref_re.shape)
    carry_im = incoming[3].reshape(pref_re.shape)
    lead_re, lead_im = power_of(log_mag, angle, float(length // 2 + 1))
    first_re = lead_re * carry_re - lead_im * carry_im
    first_im = lead_re * carry_im + lead_im * carry_re
    held_re = held_re + fade * first_re[:, None, :]
    held_im = held_im + fade * first_im[:, None, :]
    total_re = up_re * held_re - up_im * held_im
    total_im = up_re * held_im + up_im * held_re
    activated = read_out(total_re, total_im, own_inputs, c_re, c_im, d_skip)
    piece = gather_directly(activated, "tp", 1)
    mix_lin = jnp.dot(piece, w_lin, preferred_element_type=jnp.float32)
    mix_glu = jnp.dot(piece, w_glu, preferred_element_type=jnp.float32)
    mix_out = (mix_lin * jax.nn.sigmoid(mix_glu)).astype(jnp.bfloat16)
    normed_b = root_mean_normed(moe_in, moe_gain)
    experts = lax.axis_size(EP)
    tokens_here, choices_each = routes.shape
    capacity = 3 * choices_each * tokens_here // (2 * experts)
    flat_routes = routes.reshape(-1)
    onehot = (flat_routes[:, None] == jnp.arange(experts, dtype=jnp.int32)[None, :]).astype(
        jnp.int32
    )
    earlier_count = jnp.cumsum(onehot, axis=0) - onehot
    slot_index = jnp.sum(earlier_count * onehot, axis=1)
    target = flat_routes * capacity + slot_index
    places = jnp.arange(experts * capacity, dtype=jnp.int32)
    picked = jnp.any(
        places[:, None, None] == target.reshape(tokens_here, choices_each)[None], axis=2
    )
    picked = picked.astype(jnp.bfloat16)
    outgoing = jnp.dot(picked, normed_b, preferred_element_type=jnp.float32).astype(jnp.bfloat16)
    outgoing = outgoing.reshape(experts, capacity, normed_b.shape[1])
    gate_local = w_gate[0]
    up_local = w_up[0]
    down_local = w_down[0]
    received = lax.all_to_all(outgoing, EP, split_axis=0, concat_axis=0, tiled=True)
    senders, slots_here, features_here = received.shape
    token_rows = received.reshape(senders * slots_here, features_here)
    gate_pre = jnp.dot(token_rows, gate_local, preferred_element_type=jnp.float32)
    up_pre = jnp.dot(token_rows, up_local, preferred_element_type=jnp.float32)
    hidden = (jax.nn.silu(gate_pre) * up_pre).astype(jnp.bfloat16)
    partial_out = jnp.dot(hidden, down_local, preferred_element_type=jnp.float32).astype(
        jnp.bfloat16
    )
    partial_out = lax.optimization_barrier(partial_out)
    summed = sent_and_summed(partial_out.astype(jnp.float32).astype(jnp.bfloat16), "tp", 1)
    final_result = summed.astype(jnp.bfloat16).reshape(senders, slots_here, summed.shape[1])
    returned = lax.all_to_all(final_result, EP, split_axis=0, concat_axis=0, tiled=True)
    flat_returned = returned.reshape(experts * capacity, returned.shape[2])
    gathered = (
        flat_returned[target]
        .astype(jnp.float32)
        .reshape(tokens_here, choices_each, returned.shape[2])
    )
    moe_out = jnp.sum(gathered * route_weight[:, :, None], axis=1).astype(jnp.bfloat16)
    return (mix_out, moe_out)


def solution(mesh):
    torus = Mesh(mesh.devices.reshape(16, 2, mesh.shape["tp"]), ("ep_0", "ep_1", "tp"))
    placed = (
        P(EP, None),
        P(),
        P("tp", None),
        P("tp", None),
        P("tp"),
        P("tp", None, None),
        P("tp", None, None),
        P("tp", None, None),
        P("tp", None, None),
        P("tp"),
        P(EP, "tp"),
        P(None, "tp"),
        P(None, "tp"),
        P(EP, None),
        P(),
        P(EP, None),
        P(EP, None),
        P(EP, None, "tp"),
        P(EP, None, "tp"),
        P(EP, "tp", None),
    )
    return jax.shard_map(
        local, mesh=torus, in_specs=placed, out_specs=(P(EP, "tp"), P(EP, "tp")), check_vma=False
    )
```

```python
import functools

import jax
import jax.numpy as jnp
from jax import lax
from jax.experimental import pallas as pl
from jax.experimental.pallas import tpu as pltpu
from jax.sharding import Mesh
from jax.sharding import PartitionSpec as P

EP = ("z", "c")
TP = ("y", "x")
MESH = pl.DeviceIdType.MESH
PAD = 16
LANES = 128


EPS = 1e-06
HIGHEST = lax.Precision.HIGHEST


def root_mean_normed(values, gain):
    broadened_rows = values.astype(jnp.float32)
    inverse = lax.rsqrt(jnp.mean(broadened_rows * broadened_rows, axis=-1, keepdims=True) + EPS)
    return (broadened_rows * inverse * gain).astype(jnp.bfloat16)


def discretize(lam_re, lam_im, log_dt, b_re, b_im):
    time_step = jnp.exp(log_dt)[:, None]
    log_mag = lam_re * time_step
    angle = lam_im * time_step
    half_sine = jnp.sin(0.5 * angle)
    minus_re = jnp.expm1(log_mag) * jnp.cos(angle) - 2.0 * half_sine * half_sine
    minus_im = jnp.exp(log_mag) * jnp.sin(angle)
    denom = lam_re * lam_re + lam_im * lam_im
    coef_re = (minus_re * lam_re + minus_im * lam_im) / denom
    coef_im = (minus_im * lam_re - minus_re * lam_im) / denom
    drive_re = coef_re[..., None] * b_re - coef_im[..., None] * b_im
    drive_im = coef_re[..., None] * b_im + coef_im[..., None] * b_re
    return (log_mag, angle, drive_re, drive_im)


def block_scan(inputs, retain, log_mag, angle, drive_re, drive_im):
    length = inputs.shape[0]
    groups, states, channels = drive_re.shape
    broadened_rows = inputs.astype(jnp.float32).reshape(length, groups, channels)
    push_re = jnp.einsum("tgn,gpn->gtp", broadened_rows, drive_re, precision=HIGHEST)
    push_im = jnp.einsum("tgn,gpn->gtp", broadened_rows, drive_im, precision=HIGHEST)
    steps = jnp.arange(length, dtype=jnp.float32)
    causal = steps[:, None] >= steps[None, :]
    summed = jnp.dot(causal.astype(jnp.float32), retain, precision=HIGHEST)
    rows = summed.T
    gaps = jnp.minimum(rows[:, :, None] - rows[:, None, :], 0.0)
    kept = jnp.where(causal[None], jnp.exp(gaps), 0.0)
    centred = (steps - length // 2)[None, :, None]
    growth = log_mag[:, None, :] * centred
    turn = angle[:, None, :] * centred
    cosine = jnp.cos(turn)
    sine = jnp.sin(turn)
    up_re = jnp.exp(growth) * cosine
    up_im = jnp.exp(growth) * sine
    down_re = jnp.exp(-growth) * cosine
    down_im = -jnp.exp(-growth) * sine
    seed_re = push_re * down_re - push_im * down_im
    seed_im = push_re * down_im + push_im * down_re
    seeds = jnp.concatenate([seed_re, seed_im], axis=2)
    held = jnp.einsum("gts,gsp->gtp", kept, seeds, precision=HIGHEST)
    fade = jnp.exp(rows)[:, :, None]
    return (held[..., :states], held[..., states:], up_re, up_im, fade)


def power_of(log_mag, angle, exponent):
    magnitude = jnp.exp(log_mag * exponent)
    return (magnitude * jnp.cos(angle * exponent), magnitude * jnp.sin(angle * exponent))


def cols(index):
    return pl.ds(pl.multiple_of(index * LANES, LANES), LANES)


def exchange_kernel(
    sizes,
    target_ref,
    moe_ref,
    gain_ref,
    blend_ref,
    message_ref,
    turn_ref,
    partial_ref,
    prefix_ref,
    out_re_ref,
    out_im_ref,
    gate_hbm,
    up_hbm,
    down_hbm,
    lin_hbm,
    glu_hbm,
    mix_ref,
    moe_out_ref,
    gate_w,
    up_w,
    down_w,
    mix_w,
    outgoing,
    incoming,
    carries,
    gathered,
    parts,
    first_a,
    first_b,
    sum_a,
    sum_b,
    second_a,
    second_b,
    going_back,
    returned,
    active,
    weight_sem,
    z_sem,
    act_sem,
    ag_recv,
    ag_send,
    rs_sem,
):
    nz, nc, ny, nx, cap = sizes
    experts = nz * nc
    tp = ny * nx
    slots = experts * cap
    half = slots // 2
    mz, mc = lax.axis_index("z"), lax.axis_index("c")
    my, mx = lax.axis_index("y"), lax.axis_index("x")
    me = mz * nc + mc
    mt = my * nx + mx

    def along_z(k):
        peer = lax.rem(me + k, experts)
        return {"z": lax.div(peer, nc), "c": lax.rem(peer, nc)}

    def in_plane(k):
        peer = lax.rem(mt + k, tp)
        return {"y": lax.div(peer, nx), "x": lax.rem(peer, nx)}

    barrier = pltpu.get_barrier_semaphore()

    @pl.loop(1, experts)
    def _(k):
        pl.semaphore_signal(barrier, inc=1, device_id=along_z(k), device_id_type=MESH)

    @pl.loop(1, tp)
    def _(k):
        pl.semaphore_signal(barrier, inc=1, device_id=in_plane(k), device_id_type=MESH)

    loads = [
        pltpu.make_async_copy(gate_hbm, gate_w, weight_sem.at[0]),
        pltpu.make_async_copy(up_hbm, up_w, weight_sem.at[1]),
        pltpu.make_async_copy(down_hbm, down_w, weight_sem.at[2]),
        pltpu.make_async_copy(lin_hbm, mix_w.at[:, pl.ds(0, LANES)], weight_sem.at[3]),
        pltpu.make_async_copy(glu_hbm, mix_w.at[:, pl.ds(LANES, LANES)], weight_sem.at[4]),
    ]
    for load in loads:
        load.start()

    tokens, width = moe_ref.shape
    squares = jnp.zeros((tokens, LANES), jnp.float32)
    for f in range(tp):
        piece = moe_ref[:, f * LANES : (f + 1) * LANES].astype(jnp.float32)
        squares = squares + piece * piece
    mean = jnp.sum(squares, axis=1, keepdims=True) / width
    own = moe_ref[:, cols(mt)].astype(jnp.float32)
    normed = (own * lax.rsqrt(mean + EPS) * gain_ref[:, cols(mt)]).astype(jnp.bfloat16)
    place = lax.broadcasted_iota(jnp.int32, (experts * PAD, tokens), 0)
    picked = (place == target_ref[0:1, :]) | (place == target_ref[1:2, :])
    chosen = jnp.dot(
        picked.astype(jnp.float32).astype(jnp.bfloat16), normed, preferred_element_type=jnp.float32
    )
    outgoing[...] = chosen.astype(jnp.bfloat16).reshape(experts, PAD, LANES)
    incoming[me] = outgoing[me]
    pl.semaphore_wait(barrier, experts + tp - 2)

    def to_expert(k):
        peer = along_z(k)
        return pltpu.make_async_remote_copy(
            src_ref=outgoing.at[peer["z"] * nc + peer["c"]],
            dst_ref=incoming.at[me],
            send_sem=z_sem.at[0],
            recv_sem=z_sem.at[1],
            device_id=peer,
            device_id_type=MESH,
        )

    def to_later(k):
        return pltpu.make_async_remote_copy(
            src_ref=message_ref,
            dst_ref=carries.at[me],
            send_sem=z_sem.at[2],
            recv_sem=z_sem.at[3],
            device_id=along_z(k),
            device_id_type=MESH,
        )

    @pl.loop(1, experts)
    def _(k):
        to_expert(k).start()

    @pl.loop(1, experts)
    def _(k):
        to_later(k).start()

    def settle(ref, sem):
        pltpu.make_async_copy(ref, ref, sem).wait()

    others = pl.ds(0, experts - 1)
    settle(incoming.at[others], z_sem.at[1])

    row = lax.broadcasted_iota(jnp.int32, (slots, experts * PAD), 0)
    column = lax.broadcasted_iota(jnp.int32, (slots, experts * PAD), 1)
    origin = lax.shift_right_logical(row * 5462, 16)
    packing = column == origin * PAD + (row - origin * cap)
    packed = jnp.dot(
        packing.astype(jnp.float32).astype(jnp.bfloat16),
        incoming[...].reshape(experts * PAD, LANES),
        preferred_element_type=jnp.float32,
    ).astype(jnp.bfloat16)
    gathered[:, cols(mt)] = packed

    rows_a, rows_b = pl.ds(0, half), pl.ds(half, half)

    def piece_to(side, source, peer, at):
        rows = rows_a if side == 0 else rows_b
        block = gathered.at[rows, cols(source)]
        return pltpu.make_async_remote_copy(
            src_ref=block,
            dst_ref=block,
            send_sem=ag_send.at[at],
            recv_sem=ag_recv.at[side, source],
            device_id=peer,
            device_id_type=MESH,
        )

    sent = []
    for k in range(1, nx):
        sent.append(piece_to(0, mt, {"x": lax.rem(mx + k, nx)}, len(sent)))
        sent[-1].start()
    for k in range(1, ny):
        sent.append(piece_to(1, mt, {"y": lax.rem(my + k, ny)}, len(sent)))
        sent[-1].start()

    def forward(side, source):
        if side == 0:
            peers = [{"y": lax.rem(my + k, ny)} for k in range(1, ny)]
        else:
            peers = [{"x": lax.rem(mx + k, nx)} for k in range(1, nx)]
        for peer in peers:
            sent.append(piece_to(side, source, peer, len(sent)))
            sent[-1].start()

    forward(0, mt)
    forward(1, mt)
    for k in range(1, max(nx, ny)):
        if k < nx:
            source = my * nx + lax.rem(mx + k, nx)
            piece_to(0, source, {"x": mx}, 0).wait_recv()
            forward(0, source)
        if k < ny:
            source = lax.rem(my + k, ny) * nx + mx
            piece_to(1, source, {"y": my}, 0).wait_recv()
            forward(1, source)

    settle(carries.at[others], z_sem.at[3])
    stay, swap = turn_ref[0], turn_ref[1]

    def absorb(j, state):
        turned = stay * state + swap * pltpu.roll(state, 4, 0)
        return jnp.where(j < me, carries[j, 0:8, :] + carries[j, 8:16, :] * turned, state)

    carries[me] = message_ref[...]
    state = lax.fori_loop(0, experts, absorb, jnp.zeros((8, LANES), jnp.float32))
    carry_re = jnp.concatenate([state[i : i + 1, :] for i in range(4)], axis=1)
    carry_im = jnp.concatenate([state[i : i + 1, :] for i in range(4, 8)], axis=1)
    out_re, out_im = out_re_ref[...], out_im_ref[...]
    reading = jnp.concatenate(
        [out_re * carry_re - out_im * carry_im, -(out_re * carry_im + out_im * carry_re)], axis=1
    )
    total = partial_ref[...] + lax.dot_general(
        prefix_ref[...],
        reading,
        (((1,), (1,)), ((), ())),
        precision=HIGHEST,
        preferred_element_type=jnp.float32,
    )
    active[:, cols(mt)] = jax.nn.gelu(total).astype(jnp.bfloat16)

    for k in range(1, ny):
        for j in range(nx):
            source = lax.rem(my + k, ny) * nx + lax.rem(mx + j, nx)
            piece_to(0, source, {"y": my}, 0).wait_recv()
    for k in range(1, nx):
        for j in range(ny):
            source = lax.rem(my + j, ny) * nx + lax.rem(mx + k, nx)
            piece_to(1, source, {"x": mx}, 0).wait_recv()

    for load in loads:
        load.wait()
    gate = jnp.dot(gathered[...], gate_w[...], preferred_element_type=jnp.float32)
    up = jnp.dot(gathered[...], up_w[...], preferred_element_type=jnp.float32)
    hidden = (gate * jax.nn.sigmoid(gate) * up).astype(jnp.bfloat16)
    for at in range(tp // 2):
        down = jnp.dot(
            hidden,
            down_w[:, at * 2 * LANES : (at + 1) * 2 * LANES],
            preferred_element_type=jnp.float32,
        ).astype(jnp.bfloat16)
        for i in range(2):
            f = at * 2 + i
            parts[f // nx, f % nx] = down[:, i * LANES : (i + 1) * LANES]

    def first_to(side, k):
        if side == 0:
            far = lax.rem(mx + k, nx)
            source, target, peer = parts.at[:, far, rows_a], first_a.at[mx], {"x": far}
        else:
            far = lax.rem(my + k, ny)
            source, target, peer = parts.at[far, :, rows_b], first_b.at[my], {"y": far}
        return pltpu.make_async_remote_copy(
            src_ref=source,
            dst_ref=target,
            send_sem=rs_sem.at[0, side, k],
            recv_sem=rs_sem.at[1, side, k],
            device_id=peer,
            device_id_type=MESH,
        )

    def second_to(side, k):
        if side == 0:
            far = lax.rem(my + k, ny)
            source, target, peer = sum_a.at[far], second_a.at[my], {"y": far}
        else:
            far = lax.rem(mx + k, nx)
            source, target, peer = sum_b.at[far], second_b.at[mx], {"x": far}
        return pltpu.make_async_remote_copy(
            src_ref=source,
            dst_ref=target,
            send_sem=rs_sem.at[2, side, k],
            recv_sem=rs_sem.at[3, side, k],
            device_id=peer,
            device_id_type=MESH,
        )

    for k in range(1, max(nx, ny)):
        if k < nx:
            first_to(0, k).start()
        if k < ny:
            first_to(1, k).start()
    for k in range(1, max(nx, ny)):
        if k < nx:
            first_to(0, k).wait_recv()
        if k < ny:
            first_to(1, k).wait_recv()
    for j in range(ny):
        summed = parts[j, mx, 0:half, :].astype(jnp.float32)
        for k in range(1, nx):
            summed = summed + first_a[lax.rem(mx + k, nx), j].astype(jnp.float32)
        sum_a[j] = summed.astype(jnp.bfloat16)
    for k in range(1, ny):
        second_to(0, k).start()
    for j in range(nx):
        summed = parts[my, j, half:slots, :].astype(jnp.float32)
        for k in range(1, ny):
            summed = summed + first_b[lax.rem(my + k, ny), j].astype(jnp.float32)
        sum_b[j] = summed.astype(jnp.bfloat16)
    for k in range(1, nx):
        second_to(1, k).start()

    def active_to(k):
        block = active.at[:, cols(mt)]
        return pltpu.make_async_remote_copy(
            src_ref=block,
            dst_ref=block,
            send_sem=act_sem.at[0],
            recv_sem=act_sem.at[1],
            device_id=in_plane(k),
            device_id_type=MESH,
        )

    @pl.loop(1, tp)
    def _(k):
        active_to(k).start()

    for k in range(1, ny):
        second_to(0, k).wait_recv()
    for k in range(1, nx):
        second_to(1, k).wait_recv()
    result_a = sum_a[my].astype(jnp.float32)
    for k in range(1, ny):
        result_a = result_a + second_a[lax.rem(my + k, ny)].astype(jnp.float32)
    result_b = sum_b[mx].astype(jnp.float32)
    for k in range(1, nx):
        result_b = result_b + second_b[lax.rem(mx + k, nx)].astype(jnp.float32)
    result = jnp.concatenate([result_a, result_b], axis=0).astype(jnp.bfloat16)

    row = lax.broadcasted_iota(jnp.int32, (experts * PAD, slots), 0)
    column = lax.broadcasted_iota(jnp.int32, (experts * PAD, slots), 1)
    origin = lax.shift_right_logical(row, 4)
    slot = row - origin * PAD
    spreading = (slot < cap) & (column == origin * cap + slot)
    spread = jnp.dot(
        spreading.astype(jnp.float32).astype(jnp.bfloat16),
        result,
        preferred_element_type=jnp.float32,
    )
    going_back[...] = spread.astype(jnp.bfloat16).reshape(experts, PAD, LANES)
    returned[me] = going_back[me]

    def to_owner(k):
        peer = along_z(k)
        return pltpu.make_async_remote_copy(
            src_ref=going_back.at[peer["z"] * nc + peer["c"]],
            dst_ref=returned.at[me],
            send_sem=z_sem.at[4],
            recv_sem=z_sem.at[5],
            device_id=peer,
            device_id_type=MESH,
        )

    @pl.loop(1, experts)
    def _(k):
        to_owner(k).start()

    settle(active.at[:, pl.ds(0, (tp - 1) * LANES)], act_sem.at[1])
    mixed = jnp.dot(active[...], mix_w[...], preferred_element_type=jnp.float32)
    mix_ref[...] = (mixed[:, :LANES] * jax.nn.sigmoid(mixed[:, LANES:])).astype(jnp.bfloat16)

    settle(returned.at[others], z_sem.at[5])
    moe_out_ref[...] = jnp.dot(
        blend_ref[...],
        returned[...].reshape(experts * PAD, LANES).astype(jnp.float32),
        precision=HIGHEST,
        preferred_element_type=jnp.float32,
    ).astype(jnp.bfloat16)

    settle(outgoing.at[others], z_sem.at[0])
    settle(carries.at[others], z_sem.at[2])
    settle(going_back.at[others], z_sem.at[4])
    settle(active.at[:, pl.ds(0, (tp - 1) * LANES)], act_sem.at[0])
    for copy in sent:
        copy.wait_send()
    for k in range(1, nx):
        first_to(0, k).wait_send()
        second_to(1, k).wait_send()
    for k in range(1, ny):
        first_to(1, k).wait_send()
        second_to(0, k).wait_send()


def local(
    sizes,
    mix_in,
    mix_gain,
    lam_re,
    lam_im,
    log_dt,
    b_re,
    b_im,
    c_re,
    c_im,
    d_skip,
    log_retain,
    w_lin,
    w_glu,
    moe_in,
    moe_gain,
    routes,
    route_weight,
    w_gate,
    w_up,
    w_down,
):
    nz, nc, ny, nx, capacity = sizes
    experts, tp = nz * nc, ny * nx
    normed = root_mean_normed(mix_in, mix_gain)
    channels_here = d_skip.shape[0]
    own_inputs = lax.dynamic_slice_in_dim(
        normed, lax.axis_index(TP) * channels_here, channels_here, 1
    )
    log_mag, angle, drive_re, drive_im = discretize(lam_re, lam_im, log_dt, b_re, b_im)
    held_re, held_im, up_re, up_im, fade = block_scan(
        own_inputs, log_retain, log_mag, angle, drive_re, drive_im
    )
    length = own_inputs.shape[0]
    groups, states = log_mag.shape
    local_re = up_re * held_re - up_im * held_im
    local_im = up_re * held_im + up_im * held_re
    states_both = jnp.concatenate([local_re, local_im], axis=2)
    c_both = jnp.concatenate([c_re, -c_im], axis=2)
    read = jnp.einsum("gtp,gnp->tgn", states_both, c_both, precision=HIGHEST)
    partial = read.reshape(length, channels_here) + d_skip * own_inputs.astype(jnp.float32)
    lead_re, lead_im = power_of(log_mag, angle, float(length // 2 + 1))
    pref_re = fade * (up_re * lead_re[:, None] - up_im * lead_im[:, None])
    pref_im = fade * (up_re * lead_im[:, None] + up_im * lead_re[:, None])
    prefix = jnp.concatenate([pref_re, pref_im], axis=0).transpose(1, 0, 2).reshape(length, -1)
    same = jnp.eye(groups, dtype=jnp.float32)[:, None, :, None]
    out_re = (same * c_re[:, :, None, :]).reshape(channels_here, groups * states)
    out_im = (same * c_im[:, :, None, :]).reshape(channels_here, groups * states)
    whole_re, whole_im = power_of(log_mag, angle, float(length))
    lost = jnp.broadcast_to(fade[:, -1], log_mag.shape).reshape(4, LANES)
    message = jnp.concatenate(
        [local_re[:, -1].reshape(4, LANES), local_im[:, -1].reshape(4, LANES), lost, lost], axis=0
    )
    whole_re, whole_im = whole_re.reshape(4, LANES), whole_im.reshape(4, LANES)
    turn = jnp.stack(
        [
            jnp.concatenate([whole_re, whole_re], axis=0),
            jnp.concatenate([-whole_im, whole_im], axis=0),
        ]
    )

    tokens_here, choices_each = routes.shape
    flat_routes = routes.reshape(-1)
    onehot = (flat_routes[:, None] == jnp.arange(experts, dtype=jnp.int32)[None, :]).astype(
        jnp.int32
    )
    earlier_count = jnp.cumsum(onehot, axis=0) - onehot
    slot_index = jnp.sum(earlier_count * onehot, axis=1)
    target = (flat_routes * PAD + slot_index).reshape(tokens_here, choices_each)
    places = jnp.arange(experts * PAD, dtype=jnp.int32)
    blend = jnp.sum(
        jnp.where(target[:, :, None] == places[None, None], route_weight[:, :, None], 0.0), axis=1
    )

    slots, half, width = experts * capacity, experts * capacity // 2, tp * LANES
    hidden_here = w_gate.shape[2]
    bf16 = jnp.bfloat16
    vmem = pl.BlockSpec(memory_space=pltpu.VMEM)
    hbm = pl.BlockSpec(memory_space=pl.ANY)
    return pl.pallas_call(
        functools.partial(exchange_kernel, sizes),
        out_shape=(
            jax.ShapeDtypeStruct((length, LANES), bf16),
            jax.ShapeDtypeStruct((tokens_here, LANES), bf16),
        ),
        in_specs=[vmem] * 10 + [hbm] * 5,
        out_specs=(vmem, vmem),
        scratch_shapes=[
            pltpu.VMEM((width, hidden_here), bf16),
            pltpu.VMEM((width, hidden_here), bf16),
            pltpu.VMEM((hidden_here, width), bf16),
            pltpu.VMEM((width, 2 * LANES), bf16),
            pltpu.VMEM((experts, PAD, LANES), bf16),
            pltpu.VMEM((experts, PAD, LANES), bf16),
            pltpu.VMEM((experts, 16, LANES), jnp.float32),
            pltpu.VMEM((slots, width), bf16),
            pltpu.VMEM((ny, nx, slots, LANES), bf16),
            pltpu.VMEM((nx, ny, half, LANES), bf16),
            pltpu.VMEM((ny, nx, half, LANES), bf16),
            pltpu.VMEM((ny, half, LANES), bf16),
            pltpu.VMEM((nx, half, LANES), bf16),
            pltpu.VMEM((ny, half, LANES), bf16),
            pltpu.VMEM((nx, half, LANES), bf16),
            pltpu.VMEM((experts, PAD, LANES), bf16),
            pltpu.VMEM((experts, PAD, LANES), bf16),
            pltpu.VMEM((length, width), bf16),
            pltpu.SemaphoreType.DMA((5,)),
            pltpu.SemaphoreType.DMA((6,)),
            pltpu.SemaphoreType.DMA((2,)),
            pltpu.SemaphoreType.DMA((2, tp)),
            pltpu.SemaphoreType.DMA((nx - 1 + ny - 1 + nx * (ny - 1) + ny * (nx - 1),)),
            pltpu.SemaphoreType.DMA((4, 2, max(nx, ny))),
        ],
        compiler_params=pltpu.CompilerParams(
            collective_id=0, has_side_effects=True, vmem_limit_bytes=56 * 1024 * 1024
        ),
    )(
        target.T,
        moe_in,
        moe_gain.reshape(1, -1),
        blend,
        message,
        turn,
        partial,
        prefix,
        out_re,
        out_im,
        w_gate[0],
        w_up[0],
        w_down[0],
        w_lin,
        w_glu,
    )


def solution(mesh, sizes=(16, 2, 4, 4, 12)):
    torus = Mesh(mesh.devices.reshape(sizes[:4]), ("z", "c", "y", "x"))
    placed = (
        P(EP, None),
        P(),
        P(TP, None),
        P(TP, None),
        P(TP),
        P(TP, None, None),
        P(TP, None, None),
        P(TP, None, None),
        P(TP, None, None),
        P(TP),
        P(EP, TP),
        P(None, TP),
        P(None, TP),
        P(EP, None),
        P(),
        P(EP, None),
        P(EP, None),
        P(EP, None, TP),
        P(EP, None, TP),
        P(EP, TP, None),
    )
    return jax.shard_map(
        functools.partial(local, sizes),
        mesh=torus,
        in_specs=placed,
        out_specs=(P(EP, TP), P(EP, TP)),
        check_vma=False,
    )
```

```python
import functools

import jax
import jax.numpy as jnp
from jax import lax
from jax.experimental import pallas as pl
from jax.experimental.pallas import tpu as pltpu
from jax.sharding import Mesh
from jax.sharding import PartitionSpec as P

EP = ("z", "c")
TP = ("y", "x")
MESH = pl.DeviceIdType.MESH
PAD = 16
LANES = 128


EPS = 1e-06
HIGHEST = lax.Precision.HIGHEST


def compact_terms(lam_re, lam_im, log_dt, b_re, b_im, c_re, c_im):
    time_step = jnp.exp(log_dt)[:, None]
    log_mag = lam_re * time_step
    angle = lam_im * time_step
    half_sine = jnp.sin(0.5 * angle)
    cosine, sine = jnp.cos(angle), jnp.sin(angle)
    minus_re = jnp.expm1(log_mag) * cosine - 2.0 * half_sine * half_sine
    minus_im = jnp.exp(log_mag) * sine
    denom = lam_re * lam_re + lam_im * lam_im
    coef_re = (minus_re * lam_re + minus_im * lam_im) / denom
    coef_im = (minus_im * lam_re - minus_re * lam_im) / denom
    groups, states, channels = b_re.shape
    rows = groups * channels
    flip = (0, 2, 1)
    drive_re = (coef_re[..., None] * b_re - coef_im[..., None] * b_im).transpose(flip)
    drive_im = (coef_re[..., None] * b_im + coef_im[..., None] * b_re).transpose(flip)
    drive = jnp.concatenate([drive_re, drive_im], axis=2).reshape(rows, 2 * states)
    read = jnp.concatenate([c_re, -c_im], axis=2).reshape(rows, 2 * states)
    grown, shrunk = jnp.exp(log_mag), jnp.exp(-log_mag)
    decay = jnp.stack([grown * cosine, grown * sine, shrunk * cosine, -shrunk * sine])
    return drive, read, jnp.concatenate([decay, decay], axis=2)


def cols(index):
    return pl.ds(pl.multiple_of(index * LANES, LANES), LANES)


def exchange_kernel(
    sizes,
    routes_ref,
    weight_ref,
    moe_ref,
    moe_gain_ref,
    mix_gain_ref,
    retain_ref,
    decay_ref,
    drive_ref,
    read_ref,
    skip_ref,
    mix_hbm,
    gate_hbm,
    up_hbm,
    down_hbm,
    lin_hbm,
    glu_hbm,
    mix_ref,
    moe_out_ref,
    gate_w,
    up_w,
    down_w,
    mix_w,
    mix_in,
    blend,
    powers,
    partial,
    fading,
    message,
    outgoing,
    incoming,
    carries,
    gathered,
    parts,
    first_a,
    first_b,
    sum_a,
    sum_b,
    second_a,
    second_b,
    going_back,
    returned,
    active,
    weight_sem,
    z_sem,
    act_sem,
    ag_recv,
    ag_send,
    rs_sem,
):
    nz, nc, ny, nx, cap = sizes
    experts = nz * nc
    tp = ny * nx
    slots = experts * cap
    half = slots // 2
    mz, mc = lax.axis_index("z"), lax.axis_index("c")
    my, mx = lax.axis_index("y"), lax.axis_index("x")
    me = mz * nc + mc
    mt = my * nx + mx

    def along_z(k):
        peer = lax.rem(me + k, experts)
        return {"z": lax.div(peer, nc), "c": lax.rem(peer, nc)}

    def in_plane(k):
        peer = lax.rem(mt + k, tp)
        return {"y": lax.div(peer, nx), "x": lax.rem(peer, nx)}

    barrier = pltpu.get_barrier_semaphore()

    reach = experts // 2

    @pl.loop(0, reach)
    def _(k):
        pl.semaphore_signal(barrier, inc=1, device_id=along_z(reach + k), device_id_type=MESH)

        @pl.when(k > 0)
        def _():
            pl.semaphore_signal(barrier, inc=1, device_id=along_z(reach - k), device_id_type=MESH)

    @pl.loop(1, tp)
    def _(k):
        pl.semaphore_signal(barrier, inc=1, device_id=in_plane(k), device_id_type=MESH)

    mix_load = pltpu.make_async_copy(mix_hbm, mix_in, weight_sem.at[5])
    mix_load.start()
    loads = [
        pltpu.make_async_copy(gate_hbm, gate_w, weight_sem.at[0]),
        pltpu.make_async_copy(up_hbm, up_w, weight_sem.at[1]),
        pltpu.make_async_copy(down_hbm, down_w, weight_sem.at[2]),
        pltpu.make_async_copy(lin_hbm, mix_w.at[:, pl.ds(0, LANES)], weight_sem.at[3]),
        pltpu.make_async_copy(glu_hbm, mix_w.at[:, pl.ds(LANES, LANES)], weight_sem.at[4]),
    ]
    for load in loads:
        load.start()

    tokens = moe_ref.shape[0]
    lane = lax.broadcasted_iota(jnp.int32, (tokens, LANES), 1)
    picks = [lane == routes_ref[:, k : k + 1] for k in range(2)]
    named = jnp.where(picks[0] | picks[1], 1.0, 0.0).astype(jnp.bfloat16)
    ahead = lax.broadcasted_iota(jnp.int32, (tokens, tokens), 0) > lax.broadcasted_iota(
        jnp.int32, (tokens, tokens), 1
    )
    counted = jnp.dot(
        jnp.where(ahead, 1.0, 0.0).astype(jnp.bfloat16), named, preferred_element_type=jnp.float32
    )
    targets = [
        routes_ref[:, k : k + 1].astype(jnp.float32) * PAD
        + jnp.sum(jnp.where(picks[k], counted, 0.0), axis=1, keepdims=True)
        for k in range(2)
    ]
    both = jnp.where(lane == 0, targets[0], targets[1])
    if tokens < LANES:
        both = jnp.concatenate([both] * (LANES // tokens), axis=0)
    across = jnp.transpose(both)[:, :tokens].astype(jnp.int32)
    wide = lax.broadcasted_iota(jnp.int32, (tokens, experts * PAD), 1)
    blend[...] = sum(
        jnp.where(wide == targets[k].astype(jnp.int32), weight_ref[:, k : k + 1], 0.0)
        for k in range(2)
    )

    def own_features(source, gain_ref):
        squares = jnp.zeros((source.shape[0], LANES), jnp.float32)
        for f in range(tp):
            piece = source[:, f * LANES : (f + 1) * LANES].astype(jnp.float32)
            squares = squares + piece * piece
        mean = jnp.sum(squares, axis=1, keepdims=True) / source.shape[1]
        own = source[:, cols(mt)].astype(jnp.float32)
        return (own * lax.rsqrt(mean + EPS) * gain_ref[:, cols(mt)]).astype(jnp.bfloat16)

    place = lax.broadcasted_iota(jnp.int32, (experts * PAD, tokens), 0)
    picked = (place == across[0:1, :]) | (place == across[1:2, :])
    chosen = jnp.dot(
        jnp.where(picked, 1.0, 0.0).astype(jnp.bfloat16),
        own_features(moe_ref, moe_gain_ref),
        preferred_element_type=jnp.float32,
    )
    outgoing[...] = chosen.astype(jnp.bfloat16).reshape(experts, PAD, LANES)
    incoming[me] = outgoing[me]

    mix_load.wait()
    inputs = own_features(mix_in, mix_gain_ref).astype(jnp.float32)
    length, groups = inputs.shape[0], decay_ref.shape[1]
    turn_lane = lax.broadcasted_iota(jnp.int32, (1, LANES), 1)
    sign = jnp.where(turn_lane < LANES // 2, -1.0, 1.0)

    def times(a, b):
        return (a[0] * b[0] - a[1] * b[1], a[0] * b[1] + a[1] * b[0])

    grow = [(decay_ref[0], decay_ref[1])]
    shrink = [(decay_ref[2], decay_ref[3])]
    for _ in range(7):
        grow.append(times(grow[-1], grow[-1]))
        shrink.append(times(shrink[-1], shrink[-1]))
    sixteen = lax.broadcasted_iota(jnp.int32, (16, LANES), 0)

    def ladder(bases, start, stride, g):
        low = (jnp.ones((16, LANES), jnp.float32), jnp.zeros((16, LANES), jnp.float32))
        for i in range(4):
            on = (sixteen & (1 << i)) > 0
            row = [part[g : g + 1, :] for part in bases[i]]
            low = times(low, (jnp.where(on, row[0], 1.0), jnp.where(on, row[1], 0.0)))
        high = tuple(part[g : g + 1, :] for part in start)
        step = tuple(part[g : g + 1, :] for part in stride)
        blocks = []
        for _ in range(length // 16):
            blocks.append(times(low, high))
            high = times(high, step)
        return [jnp.concatenate([b[i] for b in blocks], axis=0) for i in range(2)]

    later = lax.broadcasted_iota(jnp.int32, (length, length), 0)
    sooner = lax.broadcasted_iota(jnp.int32, (length, length), 1)
    causal = later >= sooner
    summed = jnp.dot(
        jnp.where(causal, 1.0, 0.0),
        retain_ref[...],
        precision=HIGHEST,
        preferred_element_type=jnp.float32,
    )
    summed_across = jnp.transpose(summed)
    fading[...] = jnp.exp(summed)
    group_of = lax.shift_right_logical(lax.broadcasted_iota(jnp.int32, (LANES, LANES), 0), 4)

    def reading(states, g):
        return lax.dot_general(
            states,
            jnp.where(group_of == g, read_ref[...], 0.0),
            (((1,), (1,)), ((), ())),
            precision=HIGHEST,
            preferred_element_type=jnp.float32,
        )

    total = skip_ref[...] * inputs
    for g in range(groups):
        at = g * (LANES // groups)
        push = jnp.dot(
            inputs,
            jnp.where(group_of == g, drive_ref[...], 0.0),
            precision=HIGHEST,
            preferred_element_type=jnp.float32,
        )
        down_re, down_im = ladder(shrink, grow[6], shrink[4], g)
        seed = push * down_re + pltpu.roll(push, LANES // 2, 1) * (down_im * sign)
        gap = jnp.minimum(summed[:, at : at + 1] - summed_across[at : at + 1, :], 0.0)
        kept = jnp.where(causal, jnp.exp(gap), 0.0)
        held = jnp.dot(kept, seed, precision=HIGHEST, preferred_element_type=jnp.float32)
        up_re, up_im = ladder(grow, shrink[6], grow[4], g)
        up_im = up_im * sign
        powers[0, g] = up_re
        powers[1, g] = up_im
        states = held * up_re + pltpu.roll(held, LANES // 2, 1) * up_im
        total = total + reading(states, g)
        message[g : g + 1, :] = states[length - 1 : length, :]
        message[groups + g : groups + g + 1, :] = jnp.broadcast_to(
            fading[length - 1 : length, at : at + 1], (1, LANES)
        )
    partial[...] = total
    lead = times(grow[6], grow[0])
    lead = (lead[0], lead[1] * sign)
    turn = (grow[7][0], grow[7][1] * sign)
    pl.semaphore_wait(barrier, experts + tp - 2)

    def to_expert(k):
        peer = along_z(k)
        return pltpu.make_async_remote_copy(
            src_ref=outgoing.at[peer["z"] * nc + peer["c"]],
            dst_ref=incoming.at[me],
            send_sem=z_sem.at[0],
            recv_sem=z_sem.at[1],
            device_id=peer,
            device_id_type=MESH,
        )

    def to_later(k):
        return pltpu.make_async_remote_copy(
            src_ref=message,
            dst_ref=carries.at[me],
            send_sem=z_sem.at[2],
            recv_sem=z_sem.at[3],
            device_id=along_z(k),
            device_id_type=MESH,
        )

    @pl.loop(1, experts)
    def _(k):
        to_expert(k).start()

    @pl.loop(1, experts)
    def _(k):
        to_later(k).start()

    def settle(ref, sem):
        pltpu.make_async_copy(ref, ref, sem).wait()

    others = pl.ds(0, experts - 1)
    settle(incoming.at[others], z_sem.at[1])

    row = lax.broadcasted_iota(jnp.int32, (slots, experts * PAD), 0)
    column = lax.broadcasted_iota(jnp.int32, (slots, experts * PAD), 1)
    origin = lax.shift_right_logical(row * 5462, 16)
    packing = column == origin * PAD + (row - origin * cap)
    packed = jnp.dot(
        packing.astype(jnp.float32).astype(jnp.bfloat16),
        incoming[...].reshape(experts * PAD, LANES),
        preferred_element_type=jnp.float32,
    ).astype(jnp.bfloat16)
    gathered[:, cols(mt)] = packed

    rows_a, rows_b = pl.ds(0, half), pl.ds(half, half)

    def piece_to(side, source, peer, at):
        rows = rows_a if side == 0 else rows_b
        block = gathered.at[rows, cols(source)]
        return pltpu.make_async_remote_copy(
            src_ref=block,
            dst_ref=block,
            send_sem=ag_send.at[at],
            recv_sem=ag_recv.at[side, source],
            device_id=peer,
            device_id_type=MESH,
        )

    sent = []
    for k in range(1, nx):
        sent.append(piece_to(0, mt, {"x": lax.rem(mx + k, nx)}, len(sent)))
        sent[-1].start()
    for k in range(1, ny):
        sent.append(piece_to(1, mt, {"y": lax.rem(my + k, ny)}, len(sent)))
        sent[-1].start()

    def forward(side, source):
        if side == 0:
            peers = [{"y": lax.rem(my + k, ny)} for k in range(1, ny)]
        else:
            peers = [{"x": lax.rem(mx + k, nx)} for k in range(1, nx)]
        for peer in peers:
            sent.append(piece_to(side, source, peer, len(sent)))
            sent[-1].start()

    forward(0, mt)
    forward(1, mt)
    for k in range(1, max(nx, ny)):
        if k < nx:
            source = my * nx + lax.rem(mx + k, nx)
            piece_to(0, source, {"x": mx}, 0).wait_recv()
            forward(0, source)
        if k < ny:
            source = lax.rem(my + k, ny) * nx + mx
            piece_to(1, source, {"y": my}, 0).wait_recv()
            forward(1, source)

    settle(carries.at[others], z_sem.at[3])
    carries[me] = message[...]
    state = crossed = jnp.zeros((groups, LANES), jnp.float32)
    for j in range(experts):
        own, left = carries[j, 0:groups, :], carries[j, groups : 2 * groups, :]
        turned = own + left * (turn[0] * state + turn[1] * crossed)
        turned_crossed = pltpu.roll(own, LANES // 2, 1) + left * (
            turn[0] * crossed - turn[1] * state
        )
        state = jnp.where(j < me, turned, state)
        crossed = jnp.where(j < me, turned_crossed, crossed)
    first = lead[0] * state + lead[1] * crossed
    first_crossed = lead[0] * crossed - lead[1] * state
    carried = jnp.zeros((length, LANES), jnp.float32)
    for g in range(groups):
        row, row_crossed = first[g : g + 1, :], first_crossed[g : g + 1, :]
        carried = carried + reading(powers[0, g] * row + powers[1, g] * row_crossed, g)
    total = partial[...] + fading[...] * carried
    active[:, cols(mt)] = jax.nn.gelu(total).astype(jnp.bfloat16)

    for k in range(1, ny):
        for j in range(nx):
            source = lax.rem(my + k, ny) * nx + lax.rem(mx + j, nx)
            piece_to(0, source, {"y": my}, 0).wait_recv()
    for k in range(1, nx):
        for j in range(ny):
            source = lax.rem(my + j, ny) * nx + lax.rem(mx + k, nx)
            piece_to(1, source, {"x": mx}, 0).wait_recv()

    for load in loads:
        load.wait()
    gate = jnp.dot(gathered[...], gate_w[...], preferred_element_type=jnp.float32)
    up = jnp.dot(gathered[...], up_w[...], preferred_element_type=jnp.float32)
    hidden = (gate * jax.nn.sigmoid(gate) * up).astype(jnp.bfloat16)
    for at in range(tp // 2):
        down = jnp.dot(
            hidden,
            down_w[:, at * 2 * LANES : (at + 1) * 2 * LANES],
            preferred_element_type=jnp.float32,
        ).astype(jnp.bfloat16)
        for i in range(2):
            f = at * 2 + i
            parts[f // nx, f % nx] = down[:, i * LANES : (i + 1) * LANES]

    def first_to(side, k):
        if side == 0:
            far = lax.rem(mx + k, nx)
            source, target, peer = parts.at[:, far, rows_a], first_a.at[mx], {"x": far}
        else:
            far = lax.rem(my + k, ny)
            source, target, peer = parts.at[far, :, rows_b], first_b.at[my], {"y": far}
        return pltpu.make_async_remote_copy(
            src_ref=source,
            dst_ref=target,
            send_sem=rs_sem.at[0, side, k],
            recv_sem=rs_sem.at[1, side, k],
            device_id=peer,
            device_id_type=MESH,
        )

    def second_to(side, k):
        if side == 0:
            far = lax.rem(my + k, ny)
            source, target, peer = sum_a.at[far], second_a.at[my], {"y": far}
        else:
            far = lax.rem(mx + k, nx)
            source, target, peer = sum_b.at[far], second_b.at[mx], {"x": far}
        return pltpu.make_async_remote_copy(
            src_ref=source,
            dst_ref=target,
            send_sem=rs_sem.at[2, side, k],
            recv_sem=rs_sem.at[3, side, k],
            device_id=peer,
            device_id_type=MESH,
        )

    for k in range(1, max(nx, ny)):
        if k < nx:
            first_to(0, k).start()
        if k < ny:
            first_to(1, k).start()
    for k in range(1, max(nx, ny)):
        if k < nx:
            first_to(0, k).wait_recv()
        if k < ny:
            first_to(1, k).wait_recv()
    for j in range(ny):
        summed = parts[j, mx, 0:half, :].astype(jnp.float32)
        for k in range(1, nx):
            summed = summed + first_a[lax.rem(mx + k, nx), j].astype(jnp.float32)
        sum_a[j] = summed.astype(jnp.bfloat16)
    for k in range(1, ny):
        second_to(0, k).start()
    for j in range(nx):
        summed = parts[my, j, half:slots, :].astype(jnp.float32)
        for k in range(1, ny):
            summed = summed + first_b[lax.rem(my + k, ny), j].astype(jnp.float32)
        sum_b[j] = summed.astype(jnp.bfloat16)
    for k in range(1, nx):
        second_to(1, k).start()

    def active_to(k):
        block = active.at[:, cols(mt)]
        return pltpu.make_async_remote_copy(
            src_ref=block,
            dst_ref=block,
            send_sem=act_sem.at[0],
            recv_sem=act_sem.at[1],
            device_id=in_plane(k),
            device_id_type=MESH,
        )

    @pl.loop(1, tp)
    def _(k):
        active_to(k).start()

    for k in range(1, ny):
        second_to(0, k).wait_recv()
    for k in range(1, nx):
        second_to(1, k).wait_recv()
    result_a = sum_a[my].astype(jnp.float32)
    for k in range(1, ny):
        result_a = result_a + second_a[lax.rem(my + k, ny)].astype(jnp.float32)
    result_b = sum_b[mx].astype(jnp.float32)
    for k in range(1, nx):
        result_b = result_b + second_b[lax.rem(mx + k, nx)].astype(jnp.float32)
    result = jnp.concatenate([result_a, result_b], axis=0).astype(jnp.bfloat16)

    row = lax.broadcasted_iota(jnp.int32, (experts * PAD, slots), 0)
    column = lax.broadcasted_iota(jnp.int32, (experts * PAD, slots), 1)
    origin = lax.shift_right_logical(row, 4)
    slot = row - origin * PAD
    spreading = (slot < cap) & (column == origin * cap + slot)
    spread = jnp.dot(
        spreading.astype(jnp.float32).astype(jnp.bfloat16),
        result,
        preferred_element_type=jnp.float32,
    )
    going_back[...] = spread.astype(jnp.bfloat16).reshape(experts, PAD, LANES)
    returned[me] = going_back[me]

    def to_owner(k):
        peer = along_z(k)
        return pltpu.make_async_remote_copy(
            src_ref=going_back.at[peer["z"] * nc + peer["c"]],
            dst_ref=returned.at[me],
            send_sem=z_sem.at[4],
            recv_sem=z_sem.at[5],
            device_id=peer,
            device_id_type=MESH,
        )

    @pl.loop(1, experts)
    def _(k):
        to_owner(k).start()

    settle(active.at[:, pl.ds(0, (tp - 1) * LANES)], act_sem.at[1])
    mixed = jnp.dot(active[...], mix_w[...], preferred_element_type=jnp.float32)
    mix_ref[...] = (mixed[:, :LANES] * jax.nn.sigmoid(mixed[:, LANES:])).astype(jnp.bfloat16)

    settle(returned.at[others], z_sem.at[5])
    moe_out_ref[...] = jnp.dot(
        blend[...],
        returned[...].reshape(experts * PAD, LANES).astype(jnp.float32),
        precision=HIGHEST,
        preferred_element_type=jnp.float32,
    ).astype(jnp.bfloat16)

    settle(outgoing.at[others], z_sem.at[0])
    settle(carries.at[others], z_sem.at[2])
    settle(going_back.at[others], z_sem.at[4])
    settle(active.at[:, pl.ds(0, (tp - 1) * LANES)], act_sem.at[0])
    for copy in sent:
        copy.wait_send()
    for k in range(1, nx):
        first_to(0, k).wait_send()
        second_to(1, k).wait_send()
    for k in range(1, ny):
        first_to(1, k).wait_send()
        second_to(0, k).wait_send()


def local(
    sizes,
    mix_in,
    mix_gain,
    lam_re,
    lam_im,
    log_dt,
    b_re,
    b_im,
    c_re,
    c_im,
    d_skip,
    log_retain,
    w_lin,
    w_glu,
    moe_in,
    moe_gain,
    routes,
    route_weight,
    w_gate,
    w_up,
    w_down,
):
    nz, nc, ny, nx, capacity = sizes
    experts, tp = nz * nc, ny * nx
    drive, read, decay = compact_terms(lam_re, lam_im, log_dt, b_re, b_im, c_re, c_im)
    groups = decay.shape[1]
    retain = jnp.repeat(log_retain, LANES // groups, axis=1)
    length, tokens_here = mix_in.shape[0], routes.shape[0]
    slots, half, width = experts * capacity, experts * capacity // 2, tp * LANES
    hidden_here = w_gate.shape[2]
    bf16 = jnp.bfloat16
    vmem = pl.BlockSpec(memory_space=pltpu.VMEM)
    hbm = pl.BlockSpec(memory_space=pl.ANY)
    return pl.pallas_call(
        functools.partial(exchange_kernel, sizes),
        out_shape=(
            jax.ShapeDtypeStruct((length, LANES), bf16),
            jax.ShapeDtypeStruct((tokens_here, LANES), bf16),
        ),
        in_specs=[vmem] * 10 + [hbm] * 6,
        out_specs=(vmem, vmem),
        scratch_shapes=[
            pltpu.VMEM((width, hidden_here), bf16),
            pltpu.VMEM((width, hidden_here), bf16),
            pltpu.VMEM((hidden_here, width), bf16),
            pltpu.VMEM((width, 2 * LANES), bf16),
            pltpu.VMEM((length, width), bf16),
            pltpu.VMEM((tokens_here, experts * PAD), jnp.float32),
            pltpu.VMEM((2, groups, length, LANES), jnp.float32),
            pltpu.VMEM((length, LANES), jnp.float32),
            pltpu.VMEM((length, LANES), jnp.float32),
            pltpu.VMEM((2 * groups, LANES), jnp.float32),
            pltpu.VMEM((experts, PAD, LANES), bf16),
            pltpu.VMEM((experts, PAD, LANES), bf16),
            pltpu.VMEM((experts, 16, LANES), jnp.float32),
            pltpu.VMEM((slots, width), bf16),
            pltpu.VMEM((ny, nx, slots, LANES), bf16),
            pltpu.VMEM((nx, ny, half, LANES), bf16),
            pltpu.VMEM((ny, nx, half, LANES), bf16),
            pltpu.VMEM((ny, half, LANES), bf16),
            pltpu.VMEM((nx, half, LANES), bf16),
            pltpu.VMEM((ny, half, LANES), bf16),
            pltpu.VMEM((nx, half, LANES), bf16),
            pltpu.VMEM((experts, PAD, LANES), bf16),
            pltpu.VMEM((experts, PAD, LANES), bf16),
            pltpu.VMEM((length, width), bf16),
            pltpu.SemaphoreType.DMA((6,)),
            pltpu.SemaphoreType.DMA((6,)),
            pltpu.SemaphoreType.DMA((2,)),
            pltpu.SemaphoreType.DMA((2, tp)),
            pltpu.SemaphoreType.DMA((nx - 1 + ny - 1 + nx * (ny - 1) + ny * (nx - 1),)),
            pltpu.SemaphoreType.DMA((4, 2, max(nx, ny))),
        ],
        compiler_params=pltpu.CompilerParams(
            collective_id=0, has_side_effects=True, vmem_limit_bytes=56 * 1024 * 1024
        ),
    )(
        routes,
        route_weight,
        moe_in,
        moe_gain.reshape(1, -1),
        mix_gain.reshape(1, -1),
        retain,
        decay,
        drive,
        read,
        d_skip.reshape(1, -1),
        mix_in,
        w_gate[0],
        w_up[0],
        w_down[0],
        w_lin,
        w_glu,
    )


def solution(mesh, sizes=(16, 2, 4, 4, 12)):
    torus = Mesh(mesh.devices.reshape(sizes[:4]), ("z", "c", "y", "x"))
    placed = (
        P(EP, None),
        P(),
        P(TP, None),
        P(TP, None),
        P(TP),
        P(TP, None, None),
        P(TP, None, None),
        P(TP, None, None),
        P(TP, None, None),
        P(TP),
        P(EP, TP),
        P(None, TP),
        P(None, TP),
        P(EP, None),
        P(),
        P(EP, None),
        P(EP, None),
        P(EP, None, TP),
        P(EP, None, TP),
        P(EP, TP, None),
    )
    return jax.shard_map(
        functools.partial(local, sizes),
        mesh=torus,
        in_specs=placed,
        out_specs=(P(EP, TP), P(EP, TP)),
        check_vma=False,
    )
```

```python
import functools

import jax
import jax.numpy as jnp
from jax import lax
from jax.experimental import pallas as pl
from jax.experimental.pallas import tpu as pltpu
from jax.sharding import Mesh
from jax.sharding import PartitionSpec as P

EP = ("z", "c")
TP = ("y", "x")
MESH = pl.DeviceIdType.MESH
PAD = 16
LANES = 128
EPS = 1e-06
HIGHEST = lax.Precision.HIGHEST


def cols(index):
    return pl.ds(pl.multiple_of(index * LANES, LANES), LANES)


def exact_dot(a, b, contract=((1,), (0,))):
    return lax.dot_general(
        a, b, (contract, ((), ())), precision=HIGHEST, preferred_element_type=jnp.float32
    )


def fast_dot(a, b):
    return jnp.dot(a, b, preferred_element_type=jnp.float32)


def ones_where(mask, dtype):
    return jnp.where(mask, 1.0, 0.0).astype(dtype)


def times(a, b):
    return (a[0] * b[0] - a[1] * b[1], a[0] * b[1] + a[1] * b[0])


def iota(shape, axis):
    return lax.broadcasted_iota(jnp.int32, shape, axis)


def exchange_kernel(sizes, count, *refs):
    nz, nc, ny, nx, cap, pieces = sizes
    experts, tp = nz * nc, ny * nx
    slots = experts * cap
    half = slots // 2
    batch = experts // pieces
    high, low = batch * cap, batch * cap // 2
    sources, refs = refs[:count], refs[count:]
    (mix_ref, moe_ref), refs = refs[:2], refs[2:]
    staged, refs = refs[: count - 2], refs[count - 2 :]
    (mix_w, blend, powers, partial, fading, message, outgoing, incoming, carries), refs = (
        refs[:9],
        refs[9:],
    )
    (gathered, parts, first_a, first_b, sum_a, sum_b, second_a, second_b), refs = refs[:8], refs[8:]
    (going_back, returned, active, load_sem, z_sent, z_recv, carry_sem, act_sem), refs = (
        refs[:8],
        refs[8:],
    )
    ag_near, ag_far, ag_sent, rs_near, rs_far, rs_sent = refs
    (routes, weights, moe_in, moe_gain, mix_in, mix_gain, retain, lam_re, lam_im), rest = (
        staged[:9],
        staged[9:],
    )
    log_dt, b_re, b_im, c_re, c_im, skip, gate_w, up_w, down_w = rest

    mz, mc = lax.axis_index("z"), lax.axis_index("c")
    my, mx = lax.axis_index("y"), lax.axis_index("x")
    me = mz * nc + mc
    mt = my * nx + mx

    loads = [
        pltpu.make_async_copy(sources[i], staged[i], load_sem.at[i]) for i in range(count - 2)
    ]
    loads += [
        pltpu.make_async_copy(
            sources[count - 2 + i], mix_w.at[:, pl.ds(i * LANES, LANES)], load_sem.at[count - 2 + i]
        )
        for i in range(2)
    ]
    for load in loads:
        load.start()

    def along_z(k):
        peer = lax.rem(me + k, experts)
        return {"z": lax.div(peer, nc), "c": lax.rem(peer, nc)}

    def in_plane(k):
        peer = lax.rem(mt + k, tp)
        return {"y": lax.div(peer, nx), "x": lax.rem(peer, nx)}

    barrier = pltpu.get_barrier_semaphore()
    reach = experts // 2

    @pl.loop(0, reach)
    def _(k):
        pl.semaphore_signal(barrier, inc=1, device_id=along_z(reach + k), device_id_type=MESH)

        @pl.when(k > 0)
        def _():
            pl.semaphore_signal(barrier, inc=1, device_id=along_z(reach - k), device_id_type=MESH)

    @pl.loop(1, tp)
    def _(k):
        pl.semaphore_signal(barrier, inc=1, device_id=in_plane(k), device_id_type=MESH)

    for load in loads[:4]:
        load.wait()
    tokens = moe_in.shape[0]
    expert_row = iota((experts, tokens), 0)
    named = [expert_row == routes[k : k + 1, :] for k in range(2)]
    ahead = iota((tokens, tokens), 0) < iota((tokens, tokens), 1)
    counted = fast_dot(
        ones_where(named[0] | named[1], jnp.bfloat16), ones_where(ahead, jnp.bfloat16)
    )
    targets = [
        routes[k : k + 1, :].astype(jnp.float32) * PAD
        + jnp.sum(jnp.where(named[k], counted, 0.0), axis=0, keepdims=True)
        for k in range(2)
    ]
    sub = iota((LANES, tokens), 0)
    rows = jnp.where(
        sub < 2,
        jnp.where(sub == 0, targets[0], targets[1]),
        jnp.where(sub == 2, weights[0:1, :], weights[1:2, :]),
    )
    down_rows = jnp.transpose(rows)
    wide = iota((tokens, experts * PAD), 1)
    blend[...] = sum(
        jnp.where(wide == down_rows[:, k : k + 1].astype(jnp.int32), down_rows[:, k + 2 : k + 3], 0.0)
        for k in range(2)
    )

    def own_features(source, gain_ref):
        squares = jnp.zeros((source.shape[0], LANES), jnp.float32)
        for f in range(tp):
            piece = source[:, f * LANES : (f + 1) * LANES].astype(jnp.float32)
            squares = squares + piece * piece
        mean = jnp.sum(squares, axis=1, keepdims=True) / source.shape[1]
        own = source[:, cols(mt)].astype(jnp.float32)
        return (own * lax.rsqrt(mean + EPS) * gain_ref[:, cols(mt)]).astype(jnp.bfloat16)

    place = iota((experts * PAD, tokens), 0)
    picked = (place == targets[0].astype(jnp.int32)) | (place == targets[1].astype(jnp.int32))
    chosen = fast_dot(ones_where(picked, jnp.bfloat16), own_features(moe_in, moe_gain))
    outgoing[...] = chosen.astype(jnp.bfloat16).reshape(experts, PAD, LANES)
    incoming[0] = outgoing[me]

    for load in loads[4:15]:
        load.wait()
    inputs = own_features(mix_in, mix_gain).astype(jnp.float32)
    length, groups = inputs.shape[0], lam_re.shape[0]
    each = LANES // groups
    time_step = jnp.exp(jnp.transpose(log_dt[...]))
    log_mag, angle = lam_re[...] * time_step, lam_im[...] * time_step
    half_sine, cosine, sine = jnp.sin(0.5 * angle), jnp.cos(angle), jnp.sin(angle)
    grown, shrunk = jnp.exp(log_mag), jnp.exp(-log_mag)
    minus_re = jnp.tanh(0.5 * log_mag) * (grown + 1.0) * cosine - 2.0 * half_sine * half_sine
    minus_im = grown * sine
    denom = lam_re[...] * lam_re[...] + lam_im[...] * lam_im[...]
    coef_re = (minus_re * lam_re[...] + minus_im * lam_im[...]) / denom
    coef_im = (minus_im * lam_re[...] - minus_re * lam_im[...]) / denom

    def per_channel(values):
        width = values.shape[1]
        return jnp.concatenate(
            [jnp.broadcast_to(values[g : g + 1, :], (each, width)) for g in range(groups)], axis=0
        )

    drive = jnp.concatenate(
        times((per_channel(coef_re), per_channel(coef_im)), (b_re[...], b_im[...])), axis=1
    )
    read = jnp.concatenate([c_re[...], -c_im[...]], axis=1)

    def twice(values):
        return jnp.concatenate([values, values], axis=1)

    grow = [(twice(grown * cosine), twice(grown * sine))]
    shrink = [(twice(shrunk * cosine), twice(-shrunk * sine))]
    for _ in range(7):
        grow.append(times(grow[-1], grow[-1]))
        shrink.append(times(shrink[-1], shrink[-1]))
    sign = jnp.where(iota((1, LANES), 1) < LANES // 2, -1.0, 1.0)
    sixteen = iota((16, LANES), 0)

    def ladder(bases, start, stride, g):
        lower = (jnp.ones((16, LANES), jnp.float32), jnp.zeros((16, LANES), jnp.float32))
        for i in range(4):
            on = (sixteen & (1 << i)) > 0
            row = [part[g : g + 1, :] for part in bases[i]]
            lower = times(lower, (jnp.where(on, row[0], 1.0), jnp.where(on, row[1], 0.0)))
        upper = tuple(part[g : g + 1, :] for part in start)
        step = tuple(part[g : g + 1, :] for part in stride)
        blocks = []
        for _ in range(length // 16):
            blocks.append(times(lower, upper))
            upper = times(upper, step)
        return [jnp.concatenate([b[i] for b in blocks], axis=0) for i in range(2)]

    later, sooner = iota((length, length), 0), iota((length, length), 1)
    causal = later >= sooner
    summed_across = exact_dot(per_channel(retain[...]), ones_where(later <= sooner, jnp.float32))
    summed = jnp.transpose(summed_across)
    fading[...] = jnp.exp(summed)
    group_of = lax.shift_right_logical(iota((LANES, LANES), 0), 4)

    def of_group(values, g):
        return jnp.where(group_of == g, values, 0.0)

    total = skip[...] * inputs
    for g in range(groups):
        at = g * each
        push = exact_dot(inputs, of_group(drive, g))
        down_re, down_im = ladder(shrink, grow[6], shrink[4], g)
        seed = push * down_re + pltpu.roll(push, LANES // 2, 1) * (down_im * sign)
        gap = jnp.minimum(summed[:, at : at + 1] - summed_across[at : at + 1, :], 0.0)
        held = exact_dot(jnp.where(causal, jnp.exp(gap), 0.0), seed)
        up_re, up_im = ladder(grow, shrink[6], grow[4], g)
        up_im = up_im * sign
        powers[0, g] = up_re
        powers[1, g] = up_im
        states = held * up_re + pltpu.roll(held, LANES // 2, 1) * up_im
        total = total + exact_dot(states, of_group(read, g), ((1,), (1,)))
        message[g : g + 1, :] = states[length - 1 : length, :]
        message[groups + g : groups + g + 1, :] = jnp.broadcast_to(
            fading[length - 1 : length, at : at + 1], (1, LANES)
        )
    partial[...] = total
    pl.semaphore_wait(barrier, experts + tp - 2)

    def settle(ref, sem):
        pltpu.make_async_copy(ref, ref, sem).wait()

    def remote(src, dst, sent, landed, peer):
        return pltpu.make_async_remote_copy(
            src_ref=src,
            dst_ref=dst,
            send_sem=sent,
            recv_sem=landed,
            device_id=peer,
            device_id_type=MESH,
        )

    def step_of(j):
        p = lax.div(j, nc)
        return lax.div(p + 1, 2) * (2 * lax.rem(p, 2) - 1)

    def at_slot(j, direction):
        z = lax.rem(mz + direction * step_of(j) + nz, nz)
        return {"z": z, "c": lax.rem(mc + lax.rem(j, nc), nc)}

    for q in range(pieces):

        @pl.loop(q * batch if q else 1, (q + 1) * batch)
        def _(j):
            peer = at_slot(j, -1)
            block = outgoing.at[peer["z"] * nc + peer["c"]]
            remote(block, incoming.at[j], z_sent.at[0], z_recv.at[q], peer).start()

    def carry_to(k):
        return remote(
            message, carries.at[me], carry_sem.at[0, k], carry_sem.at[1, me], along_z(k)
        )

    @pl.loop(1, experts)
    def _(k):
        @pl.when(me + k < experts)
        def _():
            carry_to(k).start()

    def spot(side, q):
        return pl.ds(q * high + side * low, low)

    def inner(q):
        return pl.ds(q * low, low)

    slot_row, slot_column = iota((high, batch * PAD), 0), iota((high, batch * PAD), 1)
    origin = lax.shift_right_logical(slot_row * 5462, 16)
    packing = ones_where(slot_column == origin * PAD + (slot_row - origin * cap), jnp.bfloat16)
    slot_row, slot_column = iota((batch * PAD, high), 0), iota((batch * PAD, high), 1)
    origin = lax.shift_right_logical(slot_row, 4)
    within = slot_row - origin * PAD
    spreading = ones_where((within < cap) & (slot_column == origin * cap + within), jnp.bfloat16)

    def beside(side, k):
        if side == 0:
            return {"x": lax.rem(mx + k, nx)}
        return {"y": lax.rem(my + k, ny)}

    spans = (nx, ny)

    def near_copy(side, q, k):
        block = gathered.at[spot(side, q), cols(mt)]
        return remote(block, block, ag_sent.at[0], ag_near.at[q, side, k], beside(side, k))

    def forward(side, q, source):
        for k in range(1, spans[1 - side]):
            block = gathered.at[spot(side, q), cols(source)]
            remote(block, block, ag_sent.at[0], ag_far.at[q, side], beside(1 - side, k)).start()

    def dispatch_stage(q):
        low_slot = q * batch if q else 1
        settle(incoming.at[pl.ds(low_slot, (q + 1) * batch - low_slot)], z_recv.at[q])
        blocks = incoming[q * batch : (q + 1) * batch].reshape(batch * PAD, LANES)
        packed = fast_dot(packing, blocks).astype(jnp.bfloat16)
        gathered[pl.ds(q * high, high), cols(mt)] = packed
        for side in range(2):
            for k in range(1, spans[side]):
                near_copy(side, q, k).start()
        for side in range(2):
            forward(side, q, mt)

    def forward_stage(q):
        for k in range(1, max(nx, ny)):
            for side in range(2):
                if k < spans[side]:
                    near_copy(side, q, k).wait_recv()
                    if side == 0:
                        source = my * nx + lax.rem(mx - k + nx, nx)
                    else:
                        source = lax.rem(my - k + ny, ny) * nx + mx
                    forward(side, q, source)

    def expert_stage(q):
        for side in range(2):
            distant = spans[side] * (spans[1 - side] - 1) * LANES
            settle(gathered.at[spot(side, q), pl.ds(0, distant)], ag_far.at[q, side])
        if q == 0:
            for load in loads[15:18]:
                load.wait()
        features = gathered[q * high : (q + 1) * high, :]
        gate = fast_dot(features, gate_w[...])
        up = fast_dot(features, up_w[...])
        hidden = (gate * jax.nn.sigmoid(gate) * up).astype(jnp.bfloat16)
        for at in range(tp // 2):
            down = fast_dot(hidden, down_w[:, at * 2 * LANES : (at + 1) * 2 * LANES])
            down = down.astype(jnp.bfloat16)
            for i in range(2):
                f = at * 2 + i
                parts[f // nx, f % nx, q * high : (q + 1) * high, :] = down[
                    :, i * LANES : (i + 1) * LANES
                ]
        for k in range(1, max(nx, ny)):
            for side in range(2):
                if k < spans[side]:
                    peer = beside(side, k)
                    if side == 0:
                        src, dst = parts.at[:, peer["x"], spot(0, q)], first_a.at[k - 1, :, inner(q)]
                    else:
                        src, dst = parts.at[peer["y"], :, spot(1, q)], first_b.at[k - 1, :, inner(q)]
                    remote(src, dst, rs_sent.at[side], rs_near.at[q, side], peer).start()

    def sum_stage(q):
        for side in range(2):
            firsts = (first_a, first_b)[side]
            sums = (sum_a, sum_b)[side]
            seconds = (second_a, second_b)[side]
            settle(firsts.at[:, :, inner(q)], rs_near.at[q, side])
            for j in range(spans[1 - side]):
                own = parts[j, mx, spot(0, q), :] if side == 0 else parts[my, j, spot(1, q), :]
                summed = own.astype(jnp.float32)
                for k in range(spans[side] - 1):
                    summed = summed + firsts[k, j, inner(q), :].astype(jnp.float32)
                sums[j, inner(q), :] = summed.astype(jnp.bfloat16)
            for k in range(1, spans[1 - side]):
                peer = beside(1 - side, k)
                far = peer["y"] if side == 0 else peer["x"]
                remote(
                    sums.at[far, inner(q)],
                    seconds.at[k - 1, inner(q)],
                    rs_sent.at[2 + side],
                    rs_far.at[q, side],
                    peer,
                ).start()

    def return_stage(q):
        halves = []
        for side in range(2):
            seconds = (second_a, second_b)[side]
            settle(seconds.at[:, inner(q)], rs_far.at[q, side])
            own = sum_a[my, inner(q), :] if side == 0 else sum_b[mx, inner(q), :]
            summed = own.astype(jnp.float32)
            for k in range(spans[1 - side] - 1):
                summed = summed + seconds[k, inner(q), :].astype(jnp.float32)
            halves.append(summed)
        result = jnp.concatenate(halves, axis=0).astype(jnp.bfloat16)
        spread = fast_dot(spreading, result).astype(jnp.bfloat16)
        going_back[q * batch : (q + 1) * batch] = spread.reshape(batch, PAD, LANES)
        if q == 0:
            returned[me] = going_back[0]

        @pl.loop(q * batch if q else 1, (q + 1) * batch)
        def _(j):
            remote(
                going_back.at[j], returned.at[me], z_sent.at[1], z_recv.at[pieces], at_slot(j, 1)
            ).start()

    def active_copy(k):
        block = active.at[:, cols(mt)]
        return remote(block, block, act_sem.at[0], act_sem.at[1], in_plane(k))

    def carry_stage():
        turn = (grow[7][0], grow[7][1] * sign)
        lead = times(grow[6], grow[0])
        lead = (lead[0], lead[1] * sign)

        def absorb(j, pair):
            state, crossed = pair
            slot = carries.at[j]
            remote(slot, slot, carry_sem.at[0, 0], carry_sem.at[1, j], {"z": mz}).wait_recv()
            own, left = carries[j, 0:groups, :], carries[j, groups : 2 * groups, :]
            return (
                own + left * (turn[0] * state + turn[1] * crossed),
                pltpu.roll(own, LANES // 2, 1) + left * (turn[0] * crossed - turn[1] * state),
            )

        nothing = jnp.zeros((groups, LANES), jnp.float32)
        state, crossed = lax.fori_loop(0, me, absorb, (nothing, nothing))
        first = lead[0] * state + lead[1] * crossed
        first_crossed = lead[0] * crossed - lead[1] * state
        carried = jnp.zeros((length, LANES), jnp.float32)
        for g in range(groups):
            entering = powers[0, g] * first[g : g + 1, :] + powers[1, g] * first_crossed[g : g + 1, :]
            carried = carried + exact_dot(entering, of_group(read, g), ((1,), (1,)))
        active[:, cols(mt)] = jax.nn.gelu(partial[...] + fading[...] * carried).astype(jnp.bfloat16)

    for q in range(pieces):
        dispatch_stage(q)
        if q:
            forward_stage(q - 1)
    forward_stage(pieces - 1)
    carry_after = min(1, pieces - 1)
    for q in range(pieces + 2):
        if q < pieces:
            expert_stage(q)
        if q == carry_after:
            carry_stage()
        if 0 <= q - 1 < pieces:
            sum_stage(q - 1)
        if q == pieces:

            @pl.loop(1, tp)
            def _(k):
                active_copy(k).start()

        if 0 <= q - 2 < pieces:
            return_stage(q - 2)

    for load in loads[18:]:
        load.wait()
    settle(active.at[:, pl.ds(0, (tp - 1) * LANES)], act_sem.at[1])
    mixed = fast_dot(active[...], mix_w[...])
    mix_ref[...] = (mixed[:, :LANES] * jax.nn.sigmoid(mixed[:, LANES:])).astype(jnp.bfloat16)

    others = pl.ds(0, experts - 1)
    settle(returned.at[others], z_recv.at[pieces])
    every = returned[...].reshape(experts * PAD, LANES).astype(jnp.float32)
    moe_ref[...] = exact_dot(blend[...], every).astype(jnp.bfloat16)

    settle(outgoing.at[others], z_sent.at[0])
    settle(going_back.at[others], z_sent.at[1])
    settle(active.at[:, pl.ds(0, (tp - 1) * LANES)], act_sem.at[0])
    settle(gathered.at[:, pl.ds(0, (tp - 1) * LANES)], ag_sent.at[0])
    for at, ref in enumerate((first_a, first_b, second_a, second_b)):
        settle(ref, rs_sent.at[at])

    @pl.loop(1, experts)
    def _(k):
        @pl.when(me + k < experts)
        def _():
            carry_to(k).wait_send()


def local(
    sizes,
    mix_in,
    mix_gain,
    lam_re,
    lam_im,
    log_dt,
    b_re,
    b_im,
    c_re,
    c_im,
    d_skip,
    log_retain,
    w_lin,
    w_glu,
    moe_in,
    moe_gain,
    routes,
    route_weight,
    w_gate,
    w_up,
    w_down,
):
    nz, nc, ny, nx, capacity, pieces = sizes
    experts, tp = nz * nc, ny * nx
    groups, states, _ = b_re.shape
    flip = (0, 2, 1)
    args = (
        routes.T,
        route_weight.T,
        moe_in,
        moe_gain.reshape(1, -1),
        mix_in,
        mix_gain.reshape(1, -1),
        log_retain.T,
        lam_re,
        lam_im,
        log_dt.reshape(1, -1),
        b_re.transpose(flip).reshape(-1, states),
        b_im.transpose(flip).reshape(-1, states),
        c_re.reshape(-1, states),
        c_im.reshape(-1, states),
        d_skip.reshape(1, -1),
        w_gate[0],
        w_up[0],
        w_down[0],
        w_lin,
        w_glu,
    )
    length, tokens = mix_in.shape[0], moe_in.shape[0]
    slots, half, width = experts * capacity, experts * capacity // 2, tp * LANES
    f32, bf16 = jnp.float32, jnp.bfloat16
    dma = pltpu.SemaphoreType.DMA
    vmem = pl.BlockSpec(memory_space=pltpu.VMEM)
    return pl.pallas_call(
        functools.partial(exchange_kernel, sizes, len(args)),
        out_shape=(
            jax.ShapeDtypeStruct((length, LANES), bf16),
            jax.ShapeDtypeStruct((tokens, LANES), bf16),
        ),
        in_specs=[pl.BlockSpec(memory_space=pl.ANY)] * len(args),
        out_specs=(vmem, vmem),
        scratch_shapes=[
            *(pltpu.VMEM(a.shape, a.dtype) for a in args[:-2]),
            pltpu.VMEM((width, 2 * LANES), bf16),
            pltpu.VMEM((tokens, experts * PAD), f32),
            pltpu.VMEM((2, groups, length, LANES), f32),
            pltpu.VMEM((length, LANES), f32),
            pltpu.VMEM((length, LANES), f32),
            pltpu.VMEM((2 * groups, LANES), f32),
            pltpu.VMEM((experts, PAD, LANES), bf16),
            pltpu.VMEM((experts, PAD, LANES), bf16),
            pltpu.VMEM((experts, 2 * groups, LANES), f32),
            pltpu.VMEM((slots, width), bf16),
            pltpu.VMEM((ny, nx, slots, LANES), bf16),
            pltpu.VMEM((nx - 1, ny, half, LANES), bf16),
            pltpu.VMEM((ny - 1, nx, half, LANES), bf16),
            pltpu.VMEM((ny, half, LANES), bf16),
            pltpu.VMEM((nx, half, LANES), bf16),
            pltpu.VMEM((ny - 1, half, LANES), bf16),
            pltpu.VMEM((nx - 1, half, LANES), bf16),
            pltpu.VMEM((experts, PAD, LANES), bf16),
            pltpu.VMEM((experts, PAD, LANES), bf16),
            pltpu.VMEM((length, width), bf16),
            dma((len(args),)),
            dma((2,)),
            dma((pieces + 1,)),
            dma((2, experts)),
            dma((2,)),
            dma((pieces, 2, max(nx, ny))),
            dma((pieces, 2)),
            dma((1,)),
            dma((pieces, 2)),
            dma((pieces, 2)),
            dma((4,)),
        ],
        compiler_params=pltpu.CompilerParams(
            collective_id=0, has_side_effects=True, vmem_limit_bytes=56 * 1024 * 1024
        ),
    )(*args)


def solution(mesh, sizes=(16, 2, 4, 4, 12, 4)):
    torus = Mesh(mesh.devices.reshape(sizes[:4]), ("z", "c", "y", "x"))
    placed = (
        P(EP, None),
        P(),
        P(TP, None),
        P(TP, None),
        P(TP),
        P(TP, None, None),
        P(TP, None, None),
        P(TP, None, None),
        P(TP, None, None),
        P(TP),
        P(EP, TP),
        P(None, TP),
        P(None, TP),
        P(EP, None),
        P(),
        P(EP, None),
        P(EP, None),
        P(EP, None, TP),
        P(EP, None, TP),
        P(EP, TP, None),
    )
    return jax.shard_map(
        functools.partial(local, sizes),
        mesh=torus,
        in_specs=placed,
        out_specs=(P(EP, TP), P(EP, TP)),
        check_vma=False,
    )
```

```python
import functools

import jax
import jax.numpy as jnp
from jax import lax
from jax.experimental import pallas as pl
from jax.experimental.pallas import tpu as pltpu
from jax.sharding import Mesh
from jax.sharding import PartitionSpec as P

EP = ("z", "c")
TP = ("y", "x")
MESH = pl.DeviceIdType.MESH
PAD = 16
LANES = 128
EPS = 1e-06
HIGHEST = lax.Precision.HIGHEST
ORDER = (
    *("D0", "D1", "F0", "D2", "F1", "D3", "K", "F2", "F3"),
    *("E1", "E2", "S1", "E3", "S2", "R1", "E0", "S3", "R2"),
    *("C", "R3", "S0", "A", "R0"),
)


def cols(index):
    return pl.ds(pl.multiple_of(index * LANES, LANES), LANES)


def exact_dot(a, b, contract=((1,), (0,))):
    return lax.dot_general(
        a, b, (contract, ((), ())), precision=HIGHEST, preferred_element_type=jnp.float32
    )


def fast_dot(a, b):
    return jnp.dot(a, b, preferred_element_type=jnp.float32)


def ones_where(mask, dtype):
    return jnp.where(mask, 1.0, 0.0).astype(dtype)


def times(a, b):
    return (a[0] * b[0] - a[1] * b[1], a[0] * b[1] + a[1] * b[0])


def iota(shape, axis):
    return lax.broadcasted_iota(jnp.int32, shape, axis)


def exchange_kernel(sizes, count, *refs):
    nz, nc, ny, nx, cap, pieces, order = sizes
    experts, tp = nz * nc, ny * nx
    slots = experts * cap
    half = slots // 2
    batch = experts // pieces
    high, low = batch * cap, batch * cap // 2
    sources, refs = refs[:count], refs[count:]
    (mix_ref, moe_ref), refs = refs[:2], refs[2:]
    staged, refs = refs[: count - 2], refs[count - 2 :]
    (mix_w, blend, powers, partial, fading, message, outgoing, incoming, carries), refs = (
        refs[:9],
        refs[9:],
    )
    (gathered, parts, first_a, first_b, sum_a, sum_b, second_a, second_b), refs = refs[:8], refs[8:]
    (going_back, returned, active, load_sem, z_sent, z_recv, carry_sem, act_sem), refs = (
        refs[:8],
        refs[8:],
    )
    ag_near, ag_far, ag_sent, rs_near, rs_far, rs_sent = refs
    (routes, weights, moe_in, moe_gain, mix_in, mix_gain, retain, lam_re, lam_im), rest = (
        staged[:9],
        staged[9:],
    )
    log_dt, b_re, b_im, c_re, c_im, skip, gate_w, up_w, down_w = rest

    mz, mc = lax.axis_index("z"), lax.axis_index("c")
    my, mx = lax.axis_index("y"), lax.axis_index("x")
    me = mz * nc + mc
    mt = my * nx + mx

    loads = [
        pltpu.make_async_copy(sources[i], staged[i], load_sem.at[i]) for i in range(count - 2)
    ]
    loads += [
        pltpu.make_async_copy(
            sources[count - 2 + i], mix_w.at[:, pl.ds(i * LANES, LANES)], load_sem.at[count - 2 + i]
        )
        for i in range(2)
    ]
    for load in loads:
        load.start()

    def along_z(k):
        peer = lax.rem(me + k, experts)
        return {"z": lax.div(peer, nc), "c": lax.rem(peer, nc)}

    def in_plane(k):
        peer = lax.rem(mt + k, tp)
        return {"y": lax.div(peer, nx), "x": lax.rem(peer, nx)}

    filled = pl.ds(0, cap)
    incoming[...] = jnp.zeros_like(incoming)
    returned[...] = jnp.zeros_like(returned)

    barrier = pltpu.get_barrier_semaphore()
    reach = experts // 2

    @pl.loop(0, reach)
    def _(k):
        pl.semaphore_signal(barrier, inc=1, device_id=along_z(reach + k), device_id_type=MESH)

        @pl.when(k > 0)
        def _():
            pl.semaphore_signal(barrier, inc=1, device_id=along_z(reach - k), device_id_type=MESH)

    @pl.loop(1, tp)
    def _(k):
        pl.semaphore_signal(barrier, inc=1, device_id=in_plane(k), device_id_type=MESH)

    for load in loads[:4]:
        load.wait()
    tokens = moe_in.shape[0]
    expert_row = iota((experts, tokens), 0)
    named = [expert_row == routes[k : k + 1, :] for k in range(2)]
    ahead = iota((tokens, tokens), 0) < iota((tokens, tokens), 1)
    counted = fast_dot(
        ones_where(named[0] | named[1], jnp.bfloat16), ones_where(ahead, jnp.bfloat16)
    )
    targets = [
        routes[k : k + 1, :].astype(jnp.float32) * PAD
        + jnp.sum(jnp.where(named[k], counted, 0.0), axis=0, keepdims=True)
        for k in range(2)
    ]
    sub = iota((LANES, tokens), 0)
    rows = jnp.where(
        sub < 2,
        jnp.where(sub == 0, targets[0], targets[1]),
        jnp.where(sub == 2, weights[0:1, :], weights[1:2, :]),
    )
    down_rows = jnp.transpose(rows)
    wide = iota((tokens, experts * PAD), 1)
    blend[...] = sum(
        jnp.where(wide == down_rows[:, k : k + 1].astype(jnp.int32), down_rows[:, k + 2 : k + 3], 0.0)
        for k in range(2)
    )

    def own_features(source, gain_ref):
        squares = jnp.zeros((source.shape[0], LANES), jnp.float32)
        for f in range(tp):
            piece = source[:, f * LANES : (f + 1) * LANES].astype(jnp.float32)
            squares = squares + piece * piece
        mean = jnp.sum(squares, axis=1, keepdims=True) / source.shape[1]
        own = source[:, cols(mt)].astype(jnp.float32)
        return (own * lax.rsqrt(mean + EPS) * gain_ref[:, cols(mt)]).astype(jnp.bfloat16)

    place = iota((experts * PAD, tokens), 0)
    picked = (place == targets[0].astype(jnp.int32)) | (place == targets[1].astype(jnp.int32))
    chosen = fast_dot(ones_where(picked, jnp.bfloat16), own_features(moe_in, moe_gain))
    outgoing[...] = chosen.astype(jnp.bfloat16).reshape(experts, PAD, LANES)
    incoming[0] = outgoing[me]

    for load in loads[4:15]:
        load.wait()
    inputs = own_features(mix_in, mix_gain).astype(jnp.float32)
    length, groups = inputs.shape[0], lam_re.shape[0]
    each = LANES // groups
    time_step = jnp.exp(jnp.transpose(log_dt[...]))
    log_mag, angle = lam_re[...] * time_step, lam_im[...] * time_step
    half_sine, cosine, sine = jnp.sin(0.5 * angle), jnp.cos(angle), jnp.sin(angle)
    grown, shrunk = jnp.exp(log_mag), jnp.exp(-log_mag)
    minus_re = jnp.tanh(0.5 * log_mag) * (grown + 1.0) * cosine - 2.0 * half_sine * half_sine
    minus_im = grown * sine
    denom = lam_re[...] * lam_re[...] + lam_im[...] * lam_im[...]
    coef_re = (minus_re * lam_re[...] + minus_im * lam_im[...]) / denom
    coef_im = (minus_im * lam_re[...] - minus_re * lam_im[...]) / denom

    def per_channel(values):
        width = values.shape[1]
        return jnp.concatenate(
            [jnp.broadcast_to(values[g : g + 1, :], (each, width)) for g in range(groups)], axis=0
        )

    drive = jnp.concatenate(
        times((per_channel(coef_re), per_channel(coef_im)), (b_re[...], b_im[...])), axis=1
    )
    read = jnp.concatenate([c_re[...], -c_im[...]], axis=1)

    def twice(values):
        return jnp.concatenate([values, values], axis=1)

    grow = [(twice(grown * cosine), twice(grown * sine))]
    shrink = [(twice(shrunk * cosine), twice(-shrunk * sine))]
    for _ in range(7):
        grow.append(times(grow[-1], grow[-1]))
        shrink.append(times(shrink[-1], shrink[-1]))
    sign = jnp.where(iota((1, LANES), 1) < LANES // 2, -1.0, 1.0)
    sixteen = iota((16, LANES), 0)

    def ladder(bases, start, stride, g):
        lower = (jnp.ones((16, LANES), jnp.float32), jnp.zeros((16, LANES), jnp.float32))
        for i in range(4):
            on = (sixteen & (1 << i)) > 0
            row = [part[g : g + 1, :] for part in bases[i]]
            lower = times(lower, (jnp.where(on, row[0], 1.0), jnp.where(on, row[1], 0.0)))
        upper = tuple(part[g : g + 1, :] for part in start)
        step = tuple(part[g : g + 1, :] for part in stride)
        blocks = []
        for _ in range(length // 16):
            blocks.append(times(lower, upper))
            upper = times(upper, step)
        return [jnp.concatenate([b[i] for b in blocks], axis=0) for i in range(2)]

    later, sooner = iota((length, length), 0), iota((length, length), 1)
    causal = later >= sooner
    summed_across = exact_dot(per_channel(retain[...]), ones_where(later <= sooner, jnp.float32))
    summed = jnp.transpose(summed_across)
    fading[...] = jnp.exp(summed)
    group_of = lax.shift_right_logical(iota((LANES, LANES), 0), 4)

    def of_group(values, g):
        return jnp.where(group_of == g, values, 0.0)

    total = skip[...] * inputs
    for g in range(groups):
        at = g * each
        push = exact_dot(inputs, of_group(drive, g))
        down_re, down_im = ladder(shrink, grow[6], shrink[4], g)
        seed = push * down_re + pltpu.roll(push, LANES // 2, 1) * (down_im * sign)
        gap = jnp.minimum(summed[:, at : at + 1] - summed_across[at : at + 1, :], 0.0)
        held = exact_dot(jnp.where(causal, jnp.exp(gap), 0.0), seed)
        up_re, up_im = ladder(grow, shrink[6], grow[4], g)
        up_im = up_im * sign
        powers[0, g] = up_re
        powers[1, g] = up_im
        states = held * up_re + pltpu.roll(held, LANES // 2, 1) * up_im
        total = total + exact_dot(states, of_group(read, g), ((1,), (1,)))
        message[g : g + 1, :] = states[length - 1 : length, :]
        message[groups + g : groups + g + 1, :] = jnp.broadcast_to(
            fading[length - 1 : length, at : at + 1], (1, LANES)
        )
    partial[...] = total
    pl.semaphore_wait(barrier, experts + tp - 2)

    def settle(ref, sem):
        pltpu.make_async_copy(ref, ref, sem).wait()

    def remote(src, dst, sent, landed, peer):
        return pltpu.make_async_remote_copy(
            src_ref=src,
            dst_ref=dst,
            send_sem=sent,
            recv_sem=landed,
            device_id=peer,
            device_id_type=MESH,
        )

    def step_of(j):
        p = lax.div(j, nc)
        return lax.div(p + 1, 2) * (2 * lax.rem(p, 2) - 1)

    def at_slot(j, direction):
        z = lax.rem(mz + direction * step_of(j) + nz, nz)
        return {"z": z, "c": lax.rem(mc + lax.rem(j, nc), nc)}

    for q in range(pieces):

        @pl.loop(q * batch if q else 1, (q + 1) * batch)
        def _(j):
            peer = at_slot(j, -1)
            block = outgoing.at[peer["z"] * nc + peer["c"], filled]
            remote(block, incoming.at[j, filled], z_sent.at[0], z_recv.at[q], peer).start()

    def carry_to(k):
        return remote(
            message, carries.at[me], carry_sem.at[0, k], carry_sem.at[1, me], along_z(k)
        )

    def carry_sends():
        @pl.loop(1, experts)
        def _(k):
            @pl.when(me + k < experts)
            def _():
                carry_to(k).start()

    def spot(side, q):
        return pl.ds(q * high + side * low, low)

    def inner(q):
        return pl.ds(q * low, low)

    slot_row, slot_column = iota((high, batch * PAD), 0), iota((high, batch * PAD), 1)
    origin = lax.shift_right_logical(slot_row * 5462, 16)
    packing = ones_where(slot_column == origin * PAD + (slot_row - origin * cap), jnp.bfloat16)
    slot_row, slot_column = iota((batch * PAD, high), 0), iota((batch * PAD, high), 1)
    origin = lax.shift_right_logical(slot_row, 4)
    within = slot_row - origin * PAD
    spreading = ones_where((within < cap) & (slot_column == origin * cap + within), jnp.bfloat16)

    def beside(side, k):
        if side == 0:
            return {"x": lax.rem(mx + k, nx)}
        return {"y": lax.rem(my + k, ny)}

    spans = (nx, ny)

    def near_copy(side, q, k):
        block = gathered.at[spot(side, q), cols(mt)]
        return remote(block, block, ag_sent.at[0], ag_near.at[q, side, k], beside(side, k))

    def forward(side, q, source):
        for k in range(1, spans[1 - side]):
            block = gathered.at[spot(side, q), cols(source)]
            remote(block, block, ag_sent.at[0], ag_far.at[q, side], beside(1 - side, k)).start()

    def dispatch_stage(q):
        low_slot = q * batch if q else 1
        settle(incoming.at[pl.ds(low_slot, (q + 1) * batch - low_slot), filled], z_recv.at[q])
        blocks = incoming[q * batch : (q + 1) * batch].reshape(batch * PAD, LANES)
        packed = fast_dot(packing, blocks).astype(jnp.bfloat16)
        gathered[pl.ds(q * high, high), cols(mt)] = packed
        for side in range(2):
            for k in range(1, spans[side]):
                near_copy(side, q, k).start()
        for side in range(2):
            forward(side, q, mt)

    def forward_stage(q):
        for k in range(1, max(nx, ny)):
            for side in range(2):
                if k < spans[side]:
                    near_copy(side, q, k).wait_recv()
                    if side == 0:
                        source = my * nx + lax.rem(mx - k + nx, nx)
                    else:
                        source = lax.rem(my - k + ny, ny) * nx + mx
                    forward(side, q, source)

    def expert_stage(q):
        for side in range(2):
            distant = spans[side] * (spans[1 - side] - 1) * LANES
            settle(gathered.at[spot(side, q), pl.ds(0, distant)], ag_far.at[q, side])
        features = gathered[q * high : (q + 1) * high, :]
        gate = fast_dot(features, gate_w[...])
        up = fast_dot(features, up_w[...])
        hidden = (gate * jax.nn.sigmoid(gate) * up).astype(jnp.bfloat16)
        for at in range(tp // 2):
            down = fast_dot(hidden, down_w[:, at * 2 * LANES : (at + 1) * 2 * LANES])
            down = down.astype(jnp.bfloat16)
            for i in range(2):
                f = at * 2 + i
                parts[f // nx, f % nx, q * high : (q + 1) * high, :] = down[
                    :, i * LANES : (i + 1) * LANES
                ]
        for k in range(1, max(nx, ny)):
            for side in range(2):
                if k < spans[side]:
                    peer = beside(side, k)
                    if side == 0:
                        src, dst = parts.at[:, peer["x"], spot(0, q)], first_a.at[k - 1, :, inner(q)]
                    else:
                        src, dst = parts.at[peer["y"], :, spot(1, q)], first_b.at[k - 1, :, inner(q)]
                    remote(src, dst, rs_sent.at[side], rs_near.at[q, side], peer).start()

    def sum_stage(q):
        for side in range(2):
            firsts = (first_a, first_b)[side]
            sums = (sum_a, sum_b)[side]
            seconds = (second_a, second_b)[side]
            settle(firsts.at[:, :, inner(q)], rs_near.at[q, side])
            for j in range(spans[1 - side]):
                own = parts[j, mx, spot(0, q), :] if side == 0 else parts[my, j, spot(1, q), :]
                summed = own.astype(jnp.float32)
                for k in range(spans[side] - 1):
                    summed = summed + firsts[k, j, inner(q), :].astype(jnp.float32)
                sums[j, inner(q), :] = summed.astype(jnp.bfloat16)
            for k in range(1, spans[1 - side]):
                peer = beside(1 - side, k)
                far = peer["y"] if side == 0 else peer["x"]
                remote(
                    sums.at[far, inner(q)],
                    seconds.at[k - 1, inner(q)],
                    rs_sent.at[2 + side],
                    rs_far.at[q, side],
                    peer,
                ).start()

    def return_stage(q):
        halves = []
        for side in range(2):
            seconds = (second_a, second_b)[side]
            settle(seconds.at[:, inner(q)], rs_far.at[q, side])
            own = sum_a[my, inner(q), :] if side == 0 else sum_b[mx, inner(q), :]
            summed = own.astype(jnp.float32)
            for k in range(spans[1 - side] - 1):
                summed = summed + seconds[k, inner(q), :].astype(jnp.float32)
            halves.append(summed)
        result = jnp.concatenate(halves, axis=0).astype(jnp.bfloat16)
        spread = fast_dot(spreading, result).astype(jnp.bfloat16)
        going_back[q * batch : (q + 1) * batch] = spread.reshape(batch, PAD, LANES)
        if q == 0:
            returned[me] = going_back[0]

        @pl.loop(q * batch if q else 1, (q + 1) * batch)
        def _(j):
            remote(
                going_back.at[j, filled],
                returned.at[me, filled],
                z_sent.at[1],
                z_recv.at[pieces],
                at_slot(j, 1),
            ).start()

    def active_copy(k):
        block = active.at[:, cols(mt)]
        return remote(block, block, act_sem.at[0], act_sem.at[1], in_plane(k))

    def carry_stage():
        turn = (grow[7][0], grow[7][1] * sign)
        lead = times(grow[6], grow[0])
        lead = (lead[0], lead[1] * sign)

        def absorb(j, pair):
            state, crossed = pair
            slot = carries.at[j]
            remote(slot, slot, carry_sem.at[0, 0], carry_sem.at[1, j], {"z": mz}).wait_recv()
            own, left = carries[j, 0:groups, :], carries[j, groups : 2 * groups, :]
            return (
                own + left * (turn[0] * state + turn[1] * crossed),
                pltpu.roll(own, LANES // 2, 1) + left * (turn[0] * crossed - turn[1] * state),
            )

        nothing = jnp.zeros((groups, LANES), jnp.float32)
        state, crossed = lax.fori_loop(0, me, absorb, (nothing, nothing))
        first = lead[0] * state + lead[1] * crossed
        first_crossed = lead[0] * crossed - lead[1] * state
        carried = jnp.zeros((length, LANES), jnp.float32)
        for g in range(groups):
            entering = powers[0, g] * first[g : g + 1, :] + powers[1, g] * first_crossed[g : g + 1, :]
            carried = carried + exact_dot(entering, of_group(read, g), ((1,), (1,)))
        active[:, cols(mt)] = jax.nn.gelu(partial[...] + fading[...] * carried).astype(jnp.bfloat16)

    def active_sends():
        @pl.loop(1, tp)
        def _(k):
            active_copy(k).start()

    stages = {
        "D": dispatch_stage,
        "F": forward_stage,
        "E": expert_stage,
        "S": sum_stage,
        "R": return_stage,
        "K": carry_sends,
        "C": carry_stage,
        "A": active_sends,
    }
    for load in loads[15:18]:
        load.wait()
    for step in order:
        stages[step[0]](*(int(q) for q in step[1:]))

    for load in loads[18:]:
        load.wait()
    settle(active.at[:, pl.ds(0, (tp - 1) * LANES)], act_sem.at[1])
    mixed = fast_dot(active[...], mix_w[...])
    mix_ref[...] = (mixed[:, :LANES] * jax.nn.sigmoid(mixed[:, LANES:])).astype(jnp.bfloat16)

    others = pl.ds(0, experts - 1)
    settle(returned.at[others, filled], z_recv.at[pieces])
    every = returned[...].reshape(experts * PAD, LANES).astype(jnp.float32)
    moe_ref[...] = exact_dot(blend[...], every).astype(jnp.bfloat16)

    settle(outgoing.at[others, filled], z_sent.at[0])
    settle(going_back.at[others, filled], z_sent.at[1])
    settle(active.at[:, pl.ds(0, (tp - 1) * LANES)], act_sem.at[0])
    settle(gathered.at[:, pl.ds(0, (tp - 1) * LANES)], ag_sent.at[0])
    for at, ref in enumerate((first_a, first_b, second_a, second_b)):
        settle(ref, rs_sent.at[at])

    @pl.loop(1, experts)
    def _(k):
        @pl.when(me + k < experts)
        def _():
            carry_to(k).wait_send()


def local(
    sizes,
    mix_in,
    mix_gain,
    lam_re,
    lam_im,
    log_dt,
    b_re,
    b_im,
    c_re,
    c_im,
    d_skip,
    log_retain,
    w_lin,
    w_glu,
    moe_in,
    moe_gain,
    routes,
    route_weight,
    w_gate,
    w_up,
    w_down,
):
    nz, nc, ny, nx, capacity, pieces, _ = sizes
    experts, tp = nz * nc, ny * nx
    groups, states, _ = b_re.shape
    flip = (0, 2, 1)
    args = (
        routes.T,
        route_weight.T,
        moe_in,
        moe_gain.reshape(1, -1),
        mix_in,
        mix_gain.reshape(1, -1),
        log_retain.T,
        lam_re,
        lam_im,
        log_dt.reshape(1, -1),
        b_re.transpose(flip).reshape(-1, states),
        b_im.transpose(flip).reshape(-1, states),
        c_re.reshape(-1, states),
        c_im.reshape(-1, states),
        d_skip.reshape(1, -1),
        w_gate[0],
        w_up[0],
        w_down[0],
        w_lin,
        w_glu,
    )
    length, tokens = mix_in.shape[0], moe_in.shape[0]
    slots, half, width = experts * capacity, experts * capacity // 2, tp * LANES
    f32, bf16 = jnp.float32, jnp.bfloat16
    dma = pltpu.SemaphoreType.DMA
    vmem = pl.BlockSpec(memory_space=pltpu.VMEM)
    return pl.pallas_call(
        functools.partial(exchange_kernel, sizes, len(args)),
        out_shape=(
            jax.ShapeDtypeStruct((length, LANES), bf16),
            jax.ShapeDtypeStruct((tokens, LANES), bf16),
        ),
        in_specs=[pl.BlockSpec(memory_space=pl.ANY)] * len(args),
        out_specs=(vmem, vmem),
        scratch_shapes=[
            *(pltpu.VMEM(a.shape, a.dtype) for a in args[:-2]),
            pltpu.VMEM((width, 2 * LANES), bf16),
            pltpu.VMEM((tokens, experts * PAD), f32),
            pltpu.VMEM((2, groups, length, LANES), f32),
            pltpu.VMEM((length, LANES), f32),
            pltpu.VMEM((length, LANES), f32),
            pltpu.VMEM((2 * groups, LANES), f32),
            pltpu.VMEM((experts, PAD, LANES), bf16),
            pltpu.VMEM((experts, PAD, LANES), bf16),
            pltpu.VMEM((experts, 2 * groups, LANES), f32),
            pltpu.VMEM((slots, width), bf16),
            pltpu.VMEM((ny, nx, slots, LANES), bf16),
            pltpu.VMEM((nx - 1, ny, half, LANES), bf16),
            pltpu.VMEM((ny - 1, nx, half, LANES), bf16),
            pltpu.VMEM((ny, half, LANES), bf16),
            pltpu.VMEM((nx, half, LANES), bf16),
            pltpu.VMEM((ny - 1, half, LANES), bf16),
            pltpu.VMEM((nx - 1, half, LANES), bf16),
            pltpu.VMEM((experts, PAD, LANES), bf16),
            pltpu.VMEM((experts, PAD, LANES), bf16),
            pltpu.VMEM((length, width), bf16),
            dma((len(args),)),
            dma((2,)),
            dma((pieces + 1,)),
            dma((2, experts)),
            dma((2,)),
            dma((pieces, 2, max(nx, ny))),
            dma((pieces, 2)),
            dma((1,)),
            dma((pieces, 2)),
            dma((pieces, 2)),
            dma((4,)),
        ],
        compiler_params=pltpu.CompilerParams(
            collective_id=0, has_side_effects=True, vmem_limit_bytes=56 * 1024 * 1024
        ),
    )(*args)


def solution(mesh, sizes=(16, 2, 4, 4, 12, 4, ORDER)):
    torus = Mesh(mesh.devices.reshape(sizes[:4]), ("z", "c", "y", "x"))
    placed = (
        P(EP, None),
        P(),
        P(TP, None),
        P(TP, None),
        P(TP),
        P(TP, None, None),
        P(TP, None, None),
        P(TP, None, None),
        P(TP, None, None),
        P(TP),
        P(EP, TP),
        P(None, TP),
        P(None, TP),
        P(EP, None),
        P(),
        P(EP, None),
        P(EP, None),
        P(EP, None, TP),
        P(EP, None, TP),
        P(EP, TP, None),
    )
    return jax.shard_map(
        functools.partial(local, sizes),
        mesh=torus,
        in_specs=placed,
        out_specs=(P(EP, TP), P(EP, TP)),
        check_vma=False,
    )
```

```python
import functools

import jax
import jax.numpy as jnp
from jax import lax
from jax.experimental import pallas as pl
from jax.experimental.pallas import tpu as pltpu
from jax.sharding import Mesh
from jax.sharding import PartitionSpec as P

EP = ("z", "c")
TP = ("y", "x")
MESH = pl.DeviceIdType.MESH
PAD = 16
LANES = 128
EPS = 1e-06
HIGHEST = lax.Precision.HIGHEST
ORDER = (
    *("D0", "D1", "F0", "D2", "K", "F1", "D3", "F2", "F3"),
    *("E1", "E2", "S1", "E3", "S2", "R1", "E0", "S3", "R2"),
    *("C", "R3", "S0", "A", "R0"),
)


def cols(index):
    return pl.ds(pl.multiple_of(index * LANES, LANES), LANES)


def exact_dot(a, b, contract=((1,), (0,))):
    return lax.dot_general(
        a, b, (contract, ((), ())), precision=HIGHEST, preferred_element_type=jnp.float32
    )


def fast_dot(a, b):
    return jnp.dot(a, b, preferred_element_type=jnp.float32)


def ones_where(mask, dtype):
    return jnp.where(mask, 1.0, 0.0).astype(dtype)


def times(a, b):
    return (a[0] * b[0] - a[1] * b[1], a[0] * b[1] + a[1] * b[0])


def iota(shape, axis):
    return lax.broadcasted_iota(jnp.int32, shape, axis)


def exchange_kernel(sizes, count, *refs):
    nz, nc, ny, nx, cap, pieces, order = sizes
    experts, tp = nz * nc, ny * nx
    slots = experts * cap
    half = slots // 2
    batch = experts // pieces
    high, low = batch * cap, batch * cap // 2
    sources, refs = refs[:count], refs[count:]
    (out_ref,), refs = refs[:1], refs[1:]
    staged, refs = refs[: count - 2], refs[count - 2 :]
    (mix_w, blend, powers, partial, fading, message, outgoing, incoming, carries), refs = (
        refs[:9],
        refs[9:],
    )
    (gathered, parts, first_a, first_b, sum_a, sum_b, second_a, second_b), refs = refs[:8], refs[8:]
    (going_back, returned, active, load_sem, z_sent, z_recv, carry_sem, act_sem), refs = (
        refs[:8],
        refs[8:],
    )
    ag_near, ag_far, ag_sent, rs_near, rs_far, rs_sent = refs
    (routes, weights, moe_in, moe_gain, mix_in, mix_gain, retain, lam_re, lam_im), rest = (
        staged[:9],
        staged[9:],
    )
    log_dt, b_re, b_im, c_re, c_im, skip, gate_w, up_w, down_w = rest

    mz, mc = lax.axis_index("z"), lax.axis_index("c")
    my, mx = lax.axis_index("y"), lax.axis_index("x")
    me = mz * nc + mc
    mt = my * nx + mx

    loads = [
        pltpu.make_async_copy(sources[i], staged[i], load_sem.at[i]) for i in range(count - 2)
    ]
    loads += [
        pltpu.make_async_copy(
            sources[count - 2 + i], mix_w.at[:, pl.ds(i * LANES, LANES)], load_sem.at[count - 2 + i]
        )
        for i in range(2)
    ]
    for load in loads:
        load.start()

    def along_z(k):
        peer = lax.rem(me + k, experts)
        return {"z": lax.div(peer, nc), "c": lax.rem(peer, nc)}

    def in_plane(k):
        peer = lax.rem(mt + k, tp)
        return {"y": lax.div(peer, nx), "x": lax.rem(peer, nx)}

    filled = pl.ds(0, cap)
    incoming[...] = jnp.zeros_like(incoming)
    returned[...] = jnp.zeros_like(returned)

    barrier = pltpu.get_barrier_semaphore()
    reach = experts // 2

    @pl.loop(0, reach)
    def _(k):
        pl.semaphore_signal(barrier, inc=1, device_id=along_z(reach + k), device_id_type=MESH)

        @pl.when(k > 0)
        def _():
            pl.semaphore_signal(barrier, inc=1, device_id=along_z(reach - k), device_id_type=MESH)

    @pl.loop(1, tp)
    def _(k):
        pl.semaphore_signal(barrier, inc=1, device_id=in_plane(k), device_id_type=MESH)

    for load in loads[:4]:
        load.wait()
    tokens = moe_in.shape[0]
    expert_row = iota((experts, tokens), 0)
    named = [expert_row == routes[k : k + 1, :] for k in range(2)]
    ahead = iota((tokens, tokens), 0) < iota((tokens, tokens), 1)
    counted = fast_dot(
        ones_where(named[0] | named[1], jnp.bfloat16), ones_where(ahead, jnp.bfloat16)
    )
    targets = [
        routes[k : k + 1, :].astype(jnp.float32) * PAD
        + jnp.sum(jnp.where(named[k], counted, 0.0), axis=0, keepdims=True)
        for k in range(2)
    ]
    sub = iota((LANES, tokens), 0)
    rows = jnp.where(
        sub < 2,
        jnp.where(sub == 0, targets[0], targets[1]),
        jnp.where(sub == 2, weights[0:1, :], weights[1:2, :]),
    )
    down_rows = jnp.transpose(rows)
    wide = iota((tokens, experts * PAD), 1)
    blend[...] = sum(
        jnp.where(wide == down_rows[:, k : k + 1].astype(jnp.int32), down_rows[:, k + 2 : k + 3], 0.0)
        for k in range(2)
    )

    def own_features(source, gain_ref):
        squares = jnp.zeros((source.shape[0], LANES), jnp.float32)
        for f in range(tp):
            piece = source[:, f * LANES : (f + 1) * LANES].astype(jnp.float32)
            squares = squares + piece * piece
        mean = jnp.sum(squares, axis=1, keepdims=True) / source.shape[1]
        own = source[:, cols(mt)].astype(jnp.float32)
        return (own * lax.rsqrt(mean + EPS) * gain_ref[:, cols(mt)]).astype(jnp.bfloat16)

    place = iota((experts * PAD, tokens), 0)
    picked = (place == targets[0].astype(jnp.int32)) | (place == targets[1].astype(jnp.int32))
    chosen = fast_dot(ones_where(picked, jnp.bfloat16), own_features(moe_in, moe_gain))
    outgoing[...] = chosen.astype(jnp.bfloat16).reshape(experts, PAD, LANES)
    incoming[0] = outgoing[me]

    for load in loads[4:15]:
        load.wait()
    inputs = own_features(mix_in, mix_gain).astype(jnp.float32)
    length, groups = inputs.shape[0], lam_re.shape[0]
    each = LANES // groups
    time_step = jnp.exp(jnp.transpose(log_dt[...]))
    log_mag, angle = lam_re[...] * time_step, lam_im[...] * time_step
    half_sine, cosine, sine = jnp.sin(0.5 * angle), jnp.cos(angle), jnp.sin(angle)
    grown, shrunk = jnp.exp(log_mag), jnp.exp(-log_mag)
    minus_re = jnp.tanh(0.5 * log_mag) * (grown + 1.0) * cosine - 2.0 * half_sine * half_sine
    minus_im = grown * sine
    denom = lam_re[...] * lam_re[...] + lam_im[...] * lam_im[...]
    coef_re = (minus_re * lam_re[...] + minus_im * lam_im[...]) / denom
    coef_im = (minus_im * lam_re[...] - minus_re * lam_im[...]) / denom

    def per_channel(values):
        width = values.shape[1]
        return jnp.concatenate(
            [jnp.broadcast_to(values[g : g + 1, :], (each, width)) for g in range(groups)], axis=0
        )

    drive = jnp.concatenate(
        times((per_channel(coef_re), per_channel(coef_im)), (b_re[...], b_im[...])), axis=1
    )
    read = jnp.concatenate([c_re[...], -c_im[...]], axis=1)

    def twice(values):
        return jnp.concatenate([values, values], axis=1)

    grow = [(twice(grown * cosine), twice(grown * sine))]
    shrink = [(twice(shrunk * cosine), twice(-shrunk * sine))]
    for _ in range(7):
        grow.append(times(grow[-1], grow[-1]))
        shrink.append(times(shrink[-1], shrink[-1]))
    sign = jnp.where(iota((1, LANES), 1) < LANES // 2, -1.0, 1.0)
    sixteen = iota((16, LANES), 0)

    def ladder(bases, start, stride, g):
        lower = (jnp.ones((16, LANES), jnp.float32), jnp.zeros((16, LANES), jnp.float32))
        for i in range(4):
            on = (sixteen & (1 << i)) > 0
            row = [part[g : g + 1, :] for part in bases[i]]
            lower = times(lower, (jnp.where(on, row[0], 1.0), jnp.where(on, row[1], 0.0)))
        upper = tuple(part[g : g + 1, :] for part in start)
        step = tuple(part[g : g + 1, :] for part in stride)
        blocks = []
        for _ in range(length // 16):
            blocks.append(times(lower, upper))
            upper = times(upper, step)
        return [jnp.concatenate([b[i] for b in blocks], axis=0) for i in range(2)]

    later, sooner = iota((length, length), 0), iota((length, length), 1)
    causal = later >= sooner
    summed_across = exact_dot(per_channel(retain[...]), ones_where(later <= sooner, jnp.float32))
    summed = jnp.transpose(summed_across)
    fading[...] = jnp.exp(summed)
    group_of = lax.shift_right_logical(iota((LANES, LANES), 0), 4)

    def of_group(values, g):
        return jnp.where(group_of == g, values, 0.0)

    total = skip[...] * inputs
    for g in range(groups):
        at = g * each
        push = exact_dot(inputs, of_group(drive, g))
        down_re, down_im = ladder(shrink, grow[6], shrink[4], g)
        seed = push * down_re + pltpu.roll(push, LANES // 2, 1) * (down_im * sign)
        gap = jnp.minimum(summed[:, at : at + 1] - summed_across[at : at + 1, :], 0.0)
        held = exact_dot(jnp.where(causal, jnp.exp(gap), 0.0), seed)
        up_re, up_im = ladder(grow, shrink[6], grow[4], g)
        up_im = up_im * sign
        powers[0, g] = up_re
        powers[1, g] = up_im
        states = held * up_re + pltpu.roll(held, LANES // 2, 1) * up_im
        total = total + exact_dot(states, of_group(read, g), ((1,), (1,)))
        message[g : g + 1, :] = states[length - 1 : length, :]
        message[groups + g : groups + g + 1, :] = jnp.broadcast_to(
            fading[length - 1 : length, at : at + 1], (1, LANES)
        )
    partial[...] = total
    pl.semaphore_wait(barrier, experts + tp - 2)

    def settle(ref, sem):
        pltpu.make_async_copy(ref, ref, sem).wait()

    def remote(src, dst, sent, landed, peer):
        return pltpu.make_async_remote_copy(
            src_ref=src,
            dst_ref=dst,
            send_sem=sent,
            recv_sem=landed,
            device_id=peer,
            device_id_type=MESH,
        )

    def step_of(j):
        p = lax.div(j, nc)
        return lax.div(p + 1, 2) * (2 * lax.rem(p, 2) - 1)

    def at_slot(j, direction):
        z = lax.rem(mz + direction * step_of(j) + nz, nz)
        return {"z": z, "c": lax.rem(mc + lax.rem(j, nc), nc)}

    for q in range(pieces):

        @pl.loop(q * batch if q else 1, (q + 1) * batch)
        def _(j):
            peer = at_slot(j, -1)
            block = outgoing.at[peer["z"] * nc + peer["c"], filled]
            remote(block, incoming.at[j, filled], z_sent.at[0], z_recv.at[q], peer).start()

    def carry_to(k):
        return remote(
            message, carries.at[me], carry_sem.at[0, k], carry_sem.at[1, me], along_z(k)
        )

    def carry_sends():
        @pl.loop(1, experts)
        def _(k):
            @pl.when(me + k < experts)
            def _():
                carry_to(k).start()

    def spot(side, q):
        return pl.ds(q * high + side * low, low)

    def inner(q):
        return pl.ds(q * low, low)

    slot_row, slot_column = iota((high, batch * PAD), 0), iota((high, batch * PAD), 1)
    origin = lax.shift_right_logical(slot_row * 5462, 16)
    packing = ones_where(slot_column == origin * PAD + (slot_row - origin * cap), jnp.bfloat16)
    slot_row, slot_column = iota((batch * PAD, high), 0), iota((batch * PAD, high), 1)
    origin = lax.shift_right_logical(slot_row, 4)
    within = slot_row - origin * PAD
    spreading = ones_where((within < cap) & (slot_column == origin * cap + within), jnp.bfloat16)

    def beside(side, k):
        if side == 0:
            return {"x": lax.rem(mx + k, nx)}
        return {"y": lax.rem(my + k, ny)}

    spans = (nx, ny)
    widest = max(nx, ny)
    nearest_first = sorted(range(1, widest), key=lambda k: min(k, widest - k))

    def near_copy(side, q, k):
        block = gathered.at[spot(side, q), cols(mt)]
        return remote(block, block, ag_sent.at[0], ag_near.at[q, side, k], beside(side, k))

    def forward(side, q, source):
        for k in range(1, spans[1 - side]):
            block = gathered.at[spot(side, q), cols(source)]
            remote(block, block, ag_sent.at[0], ag_far.at[q, side], beside(1 - side, k)).start()

    def dispatch_stage(q):
        low_slot = q * batch if q else 1
        settle(incoming.at[pl.ds(low_slot, (q + 1) * batch - low_slot), filled], z_recv.at[q])
        blocks = incoming[q * batch : (q + 1) * batch].reshape(batch * PAD, LANES)
        packed = fast_dot(packing, blocks).astype(jnp.bfloat16)
        gathered[pl.ds(q * high, high), cols(mt)] = packed
        for side in range(2):
            for k in range(1, spans[side]):
                near_copy(side, q, k).start()
        for side in range(2):
            forward(side, q, mt)

    def forward_stage(q):
        for k in nearest_first:
            for side in range(2):
                if k < spans[side]:
                    near_copy(side, q, k).wait_recv()
                    if side == 0:
                        source = my * nx + lax.rem(mx - k + nx, nx)
                    else:
                        source = lax.rem(my - k + ny, ny) * nx + mx
                    forward(side, q, source)

    def expert_stage(q):
        for side in range(2):
            distant = spans[side] * (spans[1 - side] - 1) * LANES
            settle(gathered.at[spot(side, q), pl.ds(0, distant)], ag_far.at[q, side])
        features = gathered[q * high : (q + 1) * high, :]
        gate = fast_dot(features, gate_w[...])
        up = fast_dot(features, up_w[...])
        hidden = (gate * jax.nn.sigmoid(gate) * up).astype(jnp.bfloat16)
        for at in range(tp // 2):
            down = fast_dot(hidden, down_w[:, at * 2 * LANES : (at + 1) * 2 * LANES])
            down = down.astype(jnp.bfloat16)
            for i in range(2):
                f = at * 2 + i
                parts[f // nx, f % nx, q * high : (q + 1) * high, :] = down[
                    :, i * LANES : (i + 1) * LANES
                ]
        for k in range(1, max(nx, ny)):
            for side in range(2):
                if k < spans[side]:
                    peer = beside(side, k)
                    if side == 0:
                        src, dst = parts.at[:, peer["x"], spot(0, q)], first_a.at[k - 1, :, inner(q)]
                    else:
                        src, dst = parts.at[peer["y"], :, spot(1, q)], first_b.at[k - 1, :, inner(q)]
                    remote(src, dst, rs_sent.at[side], rs_near.at[q, side], peer).start()

    def sum_stage(q):
        for side in range(2):
            firsts = (first_a, first_b)[side]
            sums = (sum_a, sum_b)[side]
            seconds = (second_a, second_b)[side]
            settle(firsts.at[:, :, inner(q)], rs_near.at[q, side])
            for j in range(spans[1 - side]):
                own = parts[j, mx, spot(0, q), :] if side == 0 else parts[my, j, spot(1, q), :]
                summed = own.astype(jnp.float32)
                for k in range(spans[side] - 1):
                    summed = summed + firsts[k, j, inner(q), :].astype(jnp.float32)
                sums[j, inner(q), :] = summed.astype(jnp.bfloat16)
            for k in range(1, spans[1 - side]):
                peer = beside(1 - side, k)
                far = peer["y"] if side == 0 else peer["x"]
                remote(
                    sums.at[far, inner(q)],
                    seconds.at[k - 1, inner(q)],
                    rs_sent.at[2 + side],
                    rs_far.at[q, side],
                    peer,
                ).start()

    def return_stage(q):
        halves = []
        for side in range(2):
            seconds = (second_a, second_b)[side]
            settle(seconds.at[:, inner(q)], rs_far.at[q, side])
            own = sum_a[my, inner(q), :] if side == 0 else sum_b[mx, inner(q), :]
            summed = own.astype(jnp.float32)
            for k in range(spans[1 - side] - 1):
                summed = summed + seconds[k, inner(q), :].astype(jnp.float32)
            halves.append(summed)
        result = jnp.concatenate(halves, axis=0).astype(jnp.bfloat16)
        spread = fast_dot(spreading, result).astype(jnp.bfloat16)
        going_back[q * batch : (q + 1) * batch] = spread.reshape(batch, PAD, LANES)
        if q == 0:
            returned[me] = going_back[0]

        @pl.loop(q * batch if q else 1, (q + 1) * batch)
        def _(j):
            remote(
                going_back.at[j, filled],
                returned.at[me, filled],
                z_sent.at[1],
                z_recv.at[pieces],
                at_slot(j, 1),
            ).start()

    def active_copy(k):
        block = active.at[:, cols(mt)]
        return remote(block, block, act_sem.at[0], act_sem.at[1], in_plane(k))

    def carry_stage():
        turn = (grow[7][0], grow[7][1] * sign)
        lead = times(grow[6], grow[0])
        lead = (lead[0], lead[1] * sign)

        def absorb(j, pair):
            state, crossed = pair
            slot = carries.at[j]
            remote(slot, slot, carry_sem.at[0, 0], carry_sem.at[1, j], {"z": mz}).wait_recv()
            own, left = carries[j, 0:groups, :], carries[j, groups : 2 * groups, :]
            return (
                own + left * (turn[0] * state + turn[1] * crossed),
                pltpu.roll(own, LANES // 2, 1) + left * (turn[0] * crossed - turn[1] * state),
            )

        nothing = jnp.zeros((groups, LANES), jnp.float32)
        state, crossed = lax.fori_loop(0, me, absorb, (nothing, nothing))
        first = lead[0] * state + lead[1] * crossed
        first_crossed = lead[0] * crossed - lead[1] * state
        carried = jnp.zeros((length, LANES), jnp.float32)
        for g in range(groups):
            entering = powers[0, g] * first[g : g + 1, :] + powers[1, g] * first_crossed[g : g + 1, :]
            carried = carried + exact_dot(entering, of_group(read, g), ((1,), (1,)))
        active[:, cols(mt)] = jax.nn.gelu(partial[...] + fading[...] * carried).astype(jnp.bfloat16)

    def active_sends():
        @pl.loop(1, tp)
        def _(k):
            active_copy(k).start()

    stages = {
        "D": dispatch_stage,
        "F": forward_stage,
        "E": expert_stage,
        "S": sum_stage,
        "R": return_stage,
        "K": carry_sends,
        "C": carry_stage,
        "A": active_sends,
    }
    for load in loads[15:18]:
        load.wait()
    for step in order:
        stages[step[0]](*(int(q) for q in step[1:]))

    for load in loads[18:]:
        load.wait()
    settle(active.at[:, pl.ds(0, (tp - 1) * LANES)], act_sem.at[1])
    mixed = fast_dot(active[...], mix_w[...])
    out_ref[0] = (mixed[:, :LANES] * jax.nn.sigmoid(mixed[:, LANES:])).astype(jnp.bfloat16)

    others = pl.ds(0, experts - 1)
    settle(returned.at[others, filled], z_recv.at[pieces])
    every = returned[...].reshape(experts * PAD, LANES).astype(jnp.float32)
    out_ref[1] = exact_dot(blend[...], every).astype(jnp.bfloat16)

    settle(outgoing.at[others, filled], z_sent.at[0])
    settle(going_back.at[others, filled], z_sent.at[1])
    settle(active.at[:, pl.ds(0, (tp - 1) * LANES)], act_sem.at[0])
    settle(gathered.at[:, pl.ds(0, (tp - 1) * LANES)], ag_sent.at[0])
    for at, ref in enumerate((first_a, first_b, second_a, second_b)):
        settle(ref, rs_sent.at[at])

    @pl.loop(1, experts)
    def _(k):
        @pl.when(me + k < experts)
        def _():
            carry_to(k).wait_send()


def local(
    sizes,
    mix_in,
    mix_gain,
    lam_re,
    lam_im,
    log_dt,
    b_re,
    b_im,
    c_re,
    c_im,
    d_skip,
    log_retain,
    w_lin,
    w_glu,
    moe_in,
    moe_gain,
    routes,
    route_weight,
    w_gate,
    w_up,
    w_down,
):
    nz, nc, ny, nx, capacity, pieces, _ = sizes
    experts, tp = nz * nc, ny * nx
    groups, states, _ = b_re.shape
    flip = (0, 2, 1)
    args = (
        routes.T,
        route_weight.T,
        moe_in,
        moe_gain.reshape(1, -1),
        mix_in,
        mix_gain.reshape(1, -1),
        log_retain.T,
        lam_re,
        lam_im,
        log_dt.reshape(1, -1),
        b_re.transpose(flip).reshape(-1, states),
        b_im.transpose(flip).reshape(-1, states),
        c_re.reshape(-1, states),
        c_im.reshape(-1, states),
        d_skip.reshape(1, -1),
        w_gate[0],
        w_up[0],
        w_down[0],
        w_lin,
        w_glu,
    )
    length, tokens = mix_in.shape[0], moe_in.shape[0]
    slots, half, width = experts * capacity, experts * capacity // 2, tp * LANES
    f32, bf16 = jnp.float32, jnp.bfloat16
    dma = pltpu.SemaphoreType.DMA
    vmem = pl.BlockSpec(memory_space=pltpu.VMEM)
    both = pl.pallas_call(
        functools.partial(exchange_kernel, sizes, len(args)),
        out_shape=jax.ShapeDtypeStruct((2, length, LANES), bf16),
        in_specs=[pl.BlockSpec(memory_space=pl.ANY)] * len(args),
        out_specs=vmem,
        scratch_shapes=[
            *(pltpu.VMEM(a.shape, a.dtype) for a in args[:-2]),
            pltpu.VMEM((width, 2 * LANES), bf16),
            pltpu.VMEM((tokens, experts * PAD), f32),
            pltpu.VMEM((2, groups, length, LANES), f32),
            pltpu.VMEM((length, LANES), f32),
            pltpu.VMEM((length, LANES), f32),
            pltpu.VMEM((2 * groups, LANES), f32),
            pltpu.VMEM((experts, PAD, LANES), bf16),
            pltpu.VMEM((experts, PAD, LANES), bf16),
            pltpu.VMEM((experts, 2 * groups, LANES), f32),
            pltpu.VMEM((slots, width), bf16),
            pltpu.VMEM((ny, nx, slots, LANES), bf16),
            pltpu.VMEM((nx - 1, ny, half, LANES), bf16),
            pltpu.VMEM((ny - 1, nx, half, LANES), bf16),
            pltpu.VMEM((ny, half, LANES), bf16),
            pltpu.VMEM((nx, half, LANES), bf16),
            pltpu.VMEM((ny - 1, half, LANES), bf16),
            pltpu.VMEM((nx - 1, half, LANES), bf16),
            pltpu.VMEM((experts, PAD, LANES), bf16),
            pltpu.VMEM((experts, PAD, LANES), bf16),
            pltpu.VMEM((length, width), bf16),
            dma((len(args),)),
            dma((2,)),
            dma((pieces + 1,)),
            dma((2, experts)),
            dma((2,)),
            dma((pieces, 2, max(nx, ny))),
            dma((pieces, 2)),
            dma((1,)),
            dma((pieces, 2)),
            dma((pieces, 2)),
            dma((4,)),
        ],
        compiler_params=pltpu.CompilerParams(
            collective_id=0, has_side_effects=True, vmem_limit_bytes=56 * 1024 * 1024
        ),
    )(*args)
    return both[0], both[1]


def solution(mesh, sizes=(16, 2, 4, 4, 12, 4, ORDER)):
    torus = Mesh(mesh.devices.reshape(sizes[:4]), ("z", "c", "y", "x"))
    placed = (
        P(EP, None),
        P(),
        P(TP, None),
        P(TP, None),
        P(TP),
        P(TP, None, None),
        P(TP, None, None),
        P(TP, None, None),
        P(TP, None, None),
        P(TP),
        P(EP, TP),
        P(None, TP),
        P(None, TP),
        P(EP, None),
        P(),
        P(EP, None),
        P(EP, None),
        P(EP, None, TP),
        P(EP, None, TP),
        P(EP, TP, None),
    )
    return jax.shard_map(
        functools.partial(local, sizes),
        mesh=torus,
        in_specs=placed,
        out_specs=(P(EP, TP), P(EP, TP)),
        check_vma=False,
    )
```
